512 devices in a mesh: ep: 32 (over z, x), tp: 16 (over y, core).
Axes of the slice: x: 4, y: 8, z: 8, core: 2. Of those that a mesh axis runs over, the one named last changes fastest.
Arguments:
- first_batch: bfloat16 [65536, 2048], P(('ep', 'tp')), may hold values from -6 to 6
- mixer_gain: float32 [2048], replicated, may hold values from 0.1 to 1.9
- mixer_in: bfloat16 [2048, 512], P(None, 'tp'), may hold values from -0.125 to 0.125
- group_maps: bfloat16 [8, 64, 64], replicated, may hold values from -0.75 to 0.75
- pool_scale: float32 [512], replicated, may hold values from 0.1 to 1.9
- mixer_out: bfloat16 [512, 2048], P('tp'), may hold values from -0.25 to 0.25
- second_batch: bfloat16 [4096, 2048], P('ep'), may hold values from -6 to 6
- expert_gain: float32 [2048], replicated, may hold values from 0.1 to 1.9
- expert_choice: int32 [4096, 2], P('ep'), may hold values from 0 to 31, all different within a row; in each aligned block of 128 rows (0 to 127, 128 to 255, ...) at most 16 rows name the same one
- route_scores: float32 [4096, 2], P('ep'), may hold values from -6 to 6
- expert_gate: bfloat16 [32, 2048, 3584], P('ep', None, 'tp'), may hold values from -0.125 to 0.125
- expert_up: bfloat16 [32, 2048, 3584], P('ep', None, 'tp'), may hold values from -0.125 to 0.125
- expert_down: bfloat16 [32, 3584, 2048], P('ep', 'tp'), may hold values from -0.09375 to 0.09375
Outputs:
- mixed_first: bfloat16 [65536, 2048], P(('ep', 'tp'))
- experts_second: bfloat16 [4096, 2048], P('ep')
The draws below stay inside these ranges and needn't reach their ends.
Inputs may be any that keep to these rules, and one draw needn't show every extreme that they name: `expert_choice`: the two entries of a row differ. Within the rows of one device (aligned blocks of 128 rows) no expert is named more than 16 times, a bound that some block reaches there.
All inputs are finite; a program needn't handle non-finite values.
Results may differ from the reference program's by a relative error of at most 0.018.
Values may be sent and summed in bfloat16 or wider, within the bound.
No kernel may reach another device: no remote copies, remote signals or barrier semaphores. Data moves between devices by JAX's collectives and lax.ppermute only.
A program may use at most 64 MiB of HBM per device.

```python
import math
import jax
import jax.numpy as jnp
import numpy as np
from jax import lax

D = 2048
POOL = 512
GROUP = 64
FF_E = 3584
TOP = 2
SEQS = 1
ROWS_B = 128
EXPERTS = 32
CAP = 16
GROUPS = 8
TOKENS_A = 65536
TOKENS_B = 4096
N_TP = 16


def block_scale(rng, extent, shards, smallest, largest):
    def one(dim, parts):
        steps = jax.random.uniform(jax.random.fold_in(jax.random.fold_in(rng, 6), dim), (parts,), jnp.float32, smallest / len(shards), largest / len(shards))
        return jnp.repeat(jnp.exp(steps), extent[dim] // parts).reshape((-1,) + (1,) * (len(extent) - dim - 1))

    level = one(*shards[0])
    for cut in shards[1:]:
        level = level * one(*cut)
    return level


def shared_out(key, own, number, rows, number_of, top, bound, skew):
    sequence = jax.random.permutation(key, number_of)
    packed, common = load_shares(number_of, rows * top, bound, skew, True), load_shares(number_of, rows * top, bound, skew, False)
    places = jnp.arange(number_of)

    def named(lengths, offset_by):
        used = int((lengths > 0).sum())
        fixed = max(1, used // 4)
        moved = fixed + (places - fixed + offset_by * (used - fixed)) % max(1, number_of - fixed)
        return jnp.zeros((number_of,), jnp.int32).at[sequence[jnp.where(places < fixed, places, moved)]].set(jnp.asarray(lengths, jnp.int32))

    lengths = jnp.where(number % 4 == 0, named(packed, number // 4), named(common, number - number // 4 - 1))
    mixed = jax.random.permutation(jax.random.fold_in(own, 3), number_of)
    source_of, receiver = mixed[0:number_of // 2 * 2:2], mixed[1:number_of // 2 * 2:2]
    room = jnp.minimum(lengths[source_of] - 1, bound - lengths[receiver]) // 2
    room = jnp.where((source_of == sequence[0]) | (receiver == sequence[0]) | (lengths[receiver] == 0), 0, jnp.maximum(room, 0))
    moved = jax.random.randint(jax.random.fold_in(own, 4), (number_of // 2,), 0, 1 << 20) % (room + 1)
    lengths = lengths.at[source_of].add(-moved).at[receiver].add(moved)
    members = jnp.searchsorted(jnp.cumsum(lengths), jnp.arange(rows * top), side="right").astype(jnp.int32)
    grid = members.reshape(top, rows).T
    grid = grid[jax.random.permutation(jax.random.fold_in(own, 1), rows)]
    offset_by = jax.random.randint(jax.random.fold_in(own, 2), (rows, 1), 0, top)
    return jnp.take_along_axis(grid, (jnp.arange(top)[None, :] + offset_by) % top, axis=1)


def load_shares(count, total, most, lean, full):
    portions = [(1 << 20) // math.isqrt(standing ** lean) + 1 for standing in range(1, count + 1)]
    largest = most if full else min(most, max(-(-total // count), total * portions[0] // sum(portions)))
    least = 1 if total - largest >= count - 1 else 0
    counts, rest = [largest] + [least] * (count - 1), total - largest - least * (count - 1)
    while rest > 0:
        free = [i for i in range(1, count) if counts[i] < largest] or [i for i in range(1, count) if counts[i] < most]
        whole, left = sum([portions[i] for i in free]), rest
        for i in free:
            extra = min(most - counts[i], max(1, left * portions[i] // whole), rest)
            counts[i] = counts[i] + extra
            rest = rest - extra
    return np.array(counts)


def noise(rng, dims, width, limit, split=(), held_as=jnp.bfloat16):
    loudness = block_scale(rng, dims, split, -0.22, 0.18) if split else 1.0
    array = jax.random.normal(rng, dims, jnp.float32) * width * loudness
    return jnp.minimum(jnp.maximum(array, -limit), limit).astype(held_as)


def setup_inputs(seed: int = 0) -> dict:
    keys = jax.random.split(jax.random.key(seed), 14)
    first_batch = noise(keys[0], (TOKENS_A, D), 1.0, 6.0, ((0, 512),))
    mixer_gain = jnp.clip(1.0 + 0.18 * jax.random.normal(keys[1], (D,), jnp.float32), 0.1, 1.9)
    mixer_in = noise(keys[2], (D, POOL), D ** -0.5, 0.125, ((1, 16),))
    group_maps = noise(keys[3], (GROUPS, GROUP, GROUP), GROUP ** -0.5, 0.75)
    pool_scale = jnp.clip(1.0 + 0.18 * jax.random.normal(keys[4], (POOL,), jnp.float32), 0.1, 1.9)
    mixer_out = noise(keys[5], (POOL, D), POOL ** -0.5, 0.25, ((0, 16),))
    second_batch = noise(keys[6], (TOKENS_B, D), 1.0, 6.0, ((0, 32),))
    expert_gain = jnp.clip(1.0 + 0.18 * jax.random.normal(keys[7], (D,), jnp.float32), 0.1, 1.9)
    expert_choice_keys = jax.random.split(jax.random.fold_in(keys[8], 1), TOKENS_B // ROWS_B)
    expert_choice_turns = jax.random.permutation(jax.random.fold_in(keys[8], 3), TOKENS_B // ROWS_B)
    expert_choice = jax.vmap(lambda own, number: shared_out(jax.random.fold_in(keys[8], 2), own, number, ROWS_B, EXPERTS, TOP, CAP, 1))(expert_choice_keys, expert_choice_turns).reshape((TOKENS_B, TOP))
    route_scores = noise(keys[9], (TOKENS_B, TOP), 1.5, 6.0, ((0, 32),), jnp.float32)
    expert_gate = noise(keys[10], (EXPERTS, D, FF_E), D ** -0.5, 0.125, ((0, 32), (2, 16)))
    expert_up = noise(keys[11], (EXPERTS, D, FF_E), D ** -0.5, 0.125, ((0, 32), (2, 16)))
    expert_down = noise(keys[12], (EXPERTS, FF_E, D), FF_E ** -0.5, 0.09375, ((0, 32), (1, 16)))
    return dict(first_batch=first_batch, mixer_gain=mixer_gain, mixer_in=mixer_in, group_maps=group_maps, pool_scale=pool_scale, mixer_out=mixer_out, second_batch=second_batch, expert_gain=expert_gain, expert_choice=expert_choice, route_scores=route_scores, expert_gate=expert_gate, expert_up=expert_up, expert_down=expert_down)


windows = (2, 4, 8, 16)
epsilon = 1e-06

def rms_scale(values, gain):
    floats = values.astype(jnp.float32)
    factor = lax.rsqrt(lax.optimization_barrier(jnp.mean(floats * floats, axis=-1, keepdims=True)) + epsilon)
    return (floats * factor * gain).astype(jnp.bfloat16)

def pool_centred(pooled_in):
    total = pooled_in.shape[0]
    seq_length = total // SEQS
    pooled_f32 = pooled_in.astype(jnp.float32).reshape(SEQS, seq_length, POOL)
    running = jnp.pad(jnp.cumsum(pooled_f32, axis=1), ((0, 0), (1, 0), (0, 0)))
    places = jnp.arange(seq_length, dtype=jnp.int32)
    pieces = []
    for group in range(POOL // GROUP):
        half_span = windows[group % 4] // 2
        upper_end = jnp.clip(places + half_span, 0, seq_length)
        lower_end = jnp.clip(places - half_span, 0, seq_length)
        group_sums = running[:, :, group * GROUP:(group + 1) * GROUP]
        window_sum = jnp.take(group_sums, upper_end, axis=1) - jnp.take(group_sums, lower_end, axis=1)
        window_count = (upper_end - lower_end).astype(jnp.float32)[None, :, None]
        pieces.append(window_sum / window_count - pooled_f32[:, :, group * GROUP:(group + 1) * GROUP])
    return jnp.concatenate(pieces, axis=-1).reshape(total, POOL).astype(jnp.bfloat16)

def reference(first_batch, mixer_gain, mixer_in, group_maps, pool_scale, mixer_out, second_batch, expert_gain, expert_choice, route_scores, expert_gate, expert_up, expert_down):
    normed_first = rms_scale(first_batch, mixer_gain)
    pooled_in = jnp.dot(normed_first, mixer_in, preferred_element_type=jnp.float32).astype(jnp.bfloat16)
    centred = pool_centred(pooled_in)
    group_count = POOL // GROUP
    grouped = jnp.einsum('tgc,gcd->tgd', centred.reshape(-1, group_count, GROUP).astype(jnp.float32), group_maps.astype(jnp.float32))
    grouped = (grouped.reshape(-1, POOL) * pool_scale).astype(jnp.bfloat16)
    mixed_first = jnp.dot(grouped, mixer_out, preferred_element_type=jnp.float32).astype(jnp.bfloat16)
    expert_count = expert_gate.shape[0]
    block_count = second_batch.shape[0] // ROWS_B
    normed_second = rms_scale(second_batch, expert_gain)
    chosen = expert_choice.reshape(block_count, ROWS_B * TOP)
    one_hot = (chosen[:, :, None] == jnp.arange(expert_count, dtype=jnp.int32)[None, None, :]).astype(jnp.int32)
    ranking = lax.optimization_barrier(jnp.sum(jnp.cumsum(one_hot, axis=1) * one_hot, axis=2)) - 1
    local_rows = jnp.arange(ROWS_B * TOP, dtype=jnp.int32) // TOP
    global_rows = local_rows[None, :] + (jnp.arange(block_count, dtype=jnp.int32) * ROWS_B)[:, None]
    block_index = jnp.arange(block_count, dtype=jnp.int32)[:, None]
    slot_place = ((chosen * block_count + block_index) * CAP + ranking).reshape(-1)
    slot_table = jnp.zeros((expert_count * block_count * CAP,), jnp.int32).at[slot_place].set(global_rows.reshape(-1) + 1)
    slot_table = slot_table.reshape(expert_count, block_count * CAP)
    split_size = FF_E // N_TP

    def one_expert(operands):
        row_index, gate_weight, up_weight, down_weight = operands
        live_rows = row_index > 0
        taken = jnp.where(live_rows[:, None], normed_second[jnp.maximum(row_index - 1, 0)], jnp.zeros((), jnp.bfloat16))
        gate_part = jnp.dot(taken, gate_weight, preferred_element_type=jnp.float32)
        up_part = jnp.dot(taken, up_weight, preferred_element_type=jnp.float32)
        hidden = (jax.nn.silu(gate_part) * up_part).astype(jnp.bfloat16)
        partial_value = jnp.einsum('rtf,tfd->trd', hidden.reshape(-1, N_TP, split_size).astype(jnp.float32), down_weight.reshape(N_TP, split_size, D).astype(jnp.float32))
        rounded = lax.optimization_barrier(partial_value.astype(jnp.bfloat16))
        return lax.optimization_barrier(jnp.sum(rounded.astype(jnp.float32), axis=0)).astype(jnp.bfloat16)
    results = lax.map(one_expert, (slot_table, expert_gate, expert_up, expert_down))
    flat_results = results.reshape(expert_count * block_count * CAP, D)
    picked = flat_results[slot_place].reshape(-1, TOP, D).astype(jnp.float32)
    weight_first = jax.nn.sigmoid(route_scores[:, 0] - route_scores[:, 1])[:, None]
    experts_second = (weight_first * picked[:, 0] + (1.0 - weight_first) * picked[:, 1]).astype(jnp.bfloat16)
    return (mixed_first, experts_second)
```

```python
import jax
import jax.numpy as jnp
from jax import lax
from jax.sharding import Mesh
from jax.sharding import PartitionSpec as P

GROUP = 64
SEQS = 1
ALL = ("z", "x", "y", "c")
EP = ("z", "x")
TP = ("y", "c")
SWAP = [(0, 1), (1, 0)]

epsilon = 1e-06


def rms_scale(values, gain):
    floats = values.astype(jnp.float32)
    factor = lax.rsqrt(jnp.mean(floats * floats, axis=-1, keepdims=True) + epsilon)
    return (floats * factor * gain).astype(jnp.bfloat16)


def extended(block, width):
    count = lax.axis_size(ALL)
    forward = [(i, i + 1) for i in range(count - 1)]
    backward = [(target, source) for source, target in forward]
    low = lax.ppermute(block[block.shape[0] - width :], ALL, forward)
    high = lax.ppermute(block[:width], ALL, backward)
    return jnp.concatenate([low, block, high], axis=0)


def mixer_half(first_batch, mixer_gain, mixer_in, group_maps, pool_scale, mixer_out):
    count_rows = first_batch.shape[0]
    share = mixer_out.shape[0]
    both = jnp.concatenate([mixer_in.T, mixer_out], axis=0)
    gathered = lax.all_gather(both, TP)
    width = gathered.shape[2]
    in_rows = gathered[:, :share].reshape(-1, width)
    out_rows = gathered[:, share:].reshape(-1, width)
    normed = rms_scale(first_batch, mixer_gain)
    pooled_in = lax.dot_general(
        normed, in_rows, (((1,), (1,)), ((), ())), preferred_element_type=jnp.float32
    ).astype(jnp.bfloat16)
    channels = pooled_in.shape[1]
    padded = extended(pooled_in, 8).astype(jnp.float32)
    devices = lax.axis_size(ALL)
    seq_length = count_rows * devices // SEQS
    first_row = lax.axis_index(ALL) * count_rows
    places = first_row + jnp.arange(count_rows, dtype=jnp.int32)
    own_seq = places // seq_length
    group_of = jnp.arange(channels, dtype=jnp.int32) // GROUP
    half_span = jnp.left_shift(jnp.ones_like(group_of), group_of % 4)
    window_sum = jnp.zeros((count_rows, channels), jnp.float32)
    window_count = jnp.zeros((count_rows, channels), jnp.float32)
    for offset in range(-8, 8):
        inside = (
            ((places + offset) // seq_length == own_seq)[:, None]
            & (offset >= -half_span)[None, :]
            & (offset < half_span)[None, :]
        )
        window_sum = window_sum + jnp.where(
            inside, padded[8 + offset : 8 + offset + count_rows], 0.0
        )
        window_count = window_count + inside.astype(jnp.float32)
    centred = (window_sum / window_count - padded[8 : 8 + count_rows]).astype(jnp.bfloat16)
    group_count = group_maps.shape[0]
    identity = jnp.eye(group_count, dtype=jnp.bfloat16)
    block_map = jnp.einsum("gcd,gh->gchd", group_maps, identity).reshape(channels, channels)
    grouped = (jnp.dot(centred, block_map, preferred_element_type=jnp.float32) * pool_scale).astype(
        jnp.bfloat16
    )
    mixed_out = jnp.dot(grouped, out_rows, preferred_element_type=jnp.float32)
    return mixed_out.astype(jnp.bfloat16)


def dot(left, right):
    return jnp.dot(left, right, preferred_element_type=jnp.float32)


def expert_half(
    second_batch, expert_gain, expert_choice, route_scores, expert_gate, expert_up, expert_down
):
    row_count, model_width = second_batch.shape
    experts = lax.axis_size(EP)
    capacity = 4 * row_count // experts
    half_slots = capacity // 2
    half_width = model_width // 2
    core = lax.axis_index("c")

    gate_own, up_own, down_own = expert_gate[0], expert_up[0], expert_down[0]
    gate_far = lax.ppermute(gate_own, "c", SWAP)
    up_far = lax.ppermute(up_own, "c", SWAP)
    down_far = lax.ppermute(down_own, "c", SWAP)

    normed = rms_scale(second_batch, expert_gain)
    expert_ids = jnp.arange(experts, dtype=jnp.int32)
    first_t = expert_choice[:, 0][None, :] == expert_ids[:, None]
    second_t = expert_choice[:, 1][None, :] == expert_ids[:, None]
    named_t = first_t | second_t
    rows = jnp.arange(row_count, dtype=jnp.int32)
    earlier_t = (rows[:, None] < rows[None, :]).astype(jnp.bfloat16)
    rank_t = dot(named_t.astype(jnp.bfloat16), earlier_t).astype(jnp.int32)
    rank_t = jnp.where(named_t, rank_t, -1)

    own_slots = core * half_slots + jnp.arange(half_slots, dtype=jnp.int32)
    spread = (rank_t[:, None, :] == own_slots[None, :, None]).astype(jnp.bfloat16)
    outgoing = dot(spread.reshape(experts * half_slots, row_count), normed).astype(jnp.bfloat16)
    outgoing = outgoing.reshape(experts, half_slots, model_width)
    arrived = lax.all_to_all(outgoing, EP, 0, 0, tiled=True)
    incoming = arrived.reshape(experts * half_slots, model_width)

    def hidden_units(gate, up):
        return (jax.nn.silu(dot(incoming, gate)) * dot(incoming, up)).astype(jnp.bfloat16)

    partial = dot(hidden_units(gate_own, up_own), down_own) + dot(
        hidden_units(gate_far, up_far), down_far
    )
    partial = partial.astype(jnp.bfloat16).reshape(experts, half_slots, 2, half_width)
    leaving = jnp.moveaxis(partial, 2, 1).reshape(2 * experts, half_slots, half_width)
    returned = lax.all_to_all(leaving, EP + ("c",), 0, 0, tiled=True)
    returned = returned.reshape(experts * capacity, half_width)

    weight_first = jax.nn.sigmoid(route_scores[:, 0] - route_scores[:, 1])[None, :]
    weight_t = jnp.where(first_t, weight_first, jnp.where(second_t, 1.0 - weight_first, 0.0))
    slots = jnp.arange(capacity, dtype=jnp.int32)
    blend_t = jnp.where(
        rank_t[:, None, :] == slots[None, :, None], weight_t[:, None, :], 0.0
    ).reshape(experts * capacity, row_count)
    high = lax.reduce_precision(blend_t, 8, 7)
    low = blend_t - high
    both = jnp.concatenate([high, low], axis=1).astype(jnp.bfloat16)
    mixed = lax.dot_general(
        both, returned, (((0,), (0,)), ((), ())), preferred_element_type=jnp.float32
    )
    blended = (mixed[:row_count] + mixed[row_count:]).astype(jnp.bfloat16)

    ring = lax.axis_size("y")
    piece = half_width // ring
    blocks = jnp.moveaxis(blended.reshape(row_count, ring, piece), 1, 0)
    pieces = lax.all_to_all(blocks, "y", 0, 0, tiled=True)
    final = jnp.sum(pieces.astype(jnp.float32), axis=0).astype(jnp.bfloat16)
    whole = lax.all_gather(final, TP)
    whole = whole.reshape(ring, 2, row_count, piece)
    return jnp.transpose(whole, (2, 1, 0, 3)).reshape(row_count, model_width)


def per_device(
    first_batch,
    mixer_gain,
    mixer_in,
    group_maps,
    pool_scale,
    mixer_out,
    second_batch,
    expert_gain,
    expert_choice,
    route_scores,
    expert_gate,
    expert_up,
    expert_down,
):
    experts_second = expert_half(
        second_batch, expert_gain, expert_choice, route_scores, expert_gate, expert_up, expert_down
    )
    mixed_first = mixer_half(first_batch, mixer_gain, mixer_in, group_maps, pool_scale, mixer_out)
    return (mixed_first, experts_second)


def solution(mesh):
    torus = Mesh(mesh.devices.reshape(8, 4, mesh.shape["tp"] // 2, 2), ALL)
    placed = (
        P(ALL, None),
        P(),
        P(None, TP),
        P(),
        P(),
        P(TP, None),
        P(EP, None),
        P(),
        P(EP, None),
        P(EP, None),
        P(EP, None, TP),
        P(EP, None, TP),
        P(EP, TP, None),
    )
    return jax.shard_map(
        per_device,
        mesh=torus,
        in_specs=placed,
        out_specs=(P(ALL, None), P(EP, None)),
        check_vma=False,
    )
```

```python
import jax
import jax.numpy as jnp
from jax import lax
from jax.experimental import pallas as pl
from jax.experimental.pallas import tpu as pltpu
from jax.sharding import Mesh
from jax.sharding import PartitionSpec as P

GROUP = 64
SEQS = 1
ALL = ("z", "x", "y", "c")
EP = ("z", "x")
TP = ("y", "c")
PARTS = 4
STACK_VMEM = 6 << 20
FFN_VMEM = 14 << 20
SWAP = [(0, 1), (1, 0)]

epsilon = 1e-06


def rms_scale(values, gain):
    floats = values.astype(jnp.float32)
    factor = lax.rsqrt(jnp.mean(floats * floats, axis=-1, keepdims=True) + epsilon)
    return (floats * factor * gain).astype(jnp.bfloat16)


def extended(block, width):
    count = lax.axis_size(ALL)
    forward = [(i, i + 1) for i in range(count - 1)]
    backward = [(target, source) for source, target in forward]
    low = lax.ppermute(block[block.shape[0] - width :], ALL, forward)
    high = lax.ppermute(block[:width], ALL, backward)
    return jnp.concatenate([low, block, high], axis=0)


def ring_gather(shard):
    size = lax.axis_size("y")
    forward = [(i, (i + 1) % size) for i in range(size)]
    backward = [(target, source) for source, target in forward]
    blocks = {0: shard}
    low = high = shard
    for step in range(1, size // 2 + 1):
        low = lax.ppermute(low, "y", forward)
        blocks[size - step] = low
        if step < size // 2:
            high = lax.ppermute(high, "y", backward)
            blocks[step] = high
    return [blocks[r] for r in range(size)]


def mixer_half(first_batch, mixer_gain, shard, group_maps, pool_scale):
    count_rows = first_batch.shape[0]
    share = shard.shape[0] // 2
    channels = pool_scale.shape[0]
    ring = lax.axis_size("y")
    blocks = ring_gather(shard)
    own = pl.pallas_call(
        stack_body,
        out_shape=jax.ShapeDtypeStruct((len(blocks) * 2 * share, shard.shape[1]), shard.dtype),
        compiler_params=pltpu.CompilerParams(vmem_limit_bytes=STACK_VMEM),
    )(*blocks)
    far = lax.ppermute(own, "c", SWAP)
    half = channels // 2
    local = jnp.arange(channels, dtype=jnp.int32)
    core = (lax.axis_index("c") + local // half) % 2
    step = (local % half) // share
    place = ((lax.axis_index("y") + step) % ring * 2 + core) * share + local % share
    order = (place[:, None] == jnp.arange(channels, dtype=jnp.int32)[None, :]).astype(jnp.bfloat16)

    normed = rms_scale(first_batch, mixer_gain)
    by_row = (((1,), (1,)), ((), ()))
    pooled_own = lax.dot_general(
        normed, own[:half], by_row, preferred_element_type=jnp.float32
    ).astype(jnp.bfloat16)
    pooled_far = lax.dot_general(
        normed, far[:half], by_row, preferred_element_type=jnp.float32
    ).astype(jnp.bfloat16)
    pooled_in = (dot(pooled_own, order[:half]) + dot(pooled_far, order[half:])).astype(jnp.bfloat16)

    padded = extended(pooled_in, 8).astype(jnp.float32)
    length = count_rows * lax.axis_size(ALL) // SEQS
    first_row = lax.axis_index(ALL) * count_rows
    places = (first_row + jnp.arange(count_rows, dtype=jnp.int32))[:, None]
    kind = (jnp.arange(channels, dtype=jnp.int32) // GROUP % 4)[None, :]
    sums = padded
    window_sum = jnp.zeros((count_rows, channels), jnp.float32)
    for k in range(4):
        span = 1 << k
        sums = sums[:-span] + sums[span:]
        window_sum = jnp.where(kind == k, sums[8 - span : 8 - span + count_rows], window_sum)
    span = jnp.left_shift(jnp.ones_like(kind), kind)
    window_count = jnp.minimum(places + span, length) - jnp.maximum(places - span, 0)
    centred = window_sum / window_count.astype(jnp.float32) - padded[8 : 8 + count_rows]
    centred = centred.astype(jnp.bfloat16)

    group_count = group_maps.shape[0]
    identity = jnp.eye(group_count, dtype=jnp.bfloat16)
    block_map = jnp.einsum("gcd,gh->gchd", group_maps, identity).reshape(channels, channels)
    grouped = (dot(centred, block_map) * pool_scale).astype(jnp.bfloat16)
    grouped = lax.dot_general(
        grouped, order, by_row, preferred_element_type=jnp.float32
    ).astype(jnp.bfloat16)
    mixed_out = dot(grouped[:, :half], own[half:]) + dot(grouped[:, half:], far[half:])
    return mixed_out.astype(jnp.bfloat16)


def on_chip():
    return pl.BlockSpec(memory_space=pltpu.VMEM)


def stack_body(*refs):
    out = refs[-1]
    half = out.shape[0] // 2
    for r, block in enumerate(refs[:-1]):
        share = block.shape[0] // 2
        out[r * share : (r + 1) * share, :] = block[:share, :]
        out[half + r * share : half + (r + 1) * share, :] = block[share:, :]


def ffn_body(rows, gate_a, up_a, down_a, gate_b, up_b, down_b, out, held, done):
    values = rows[...]
    by_row = (((1,), (1,)), ((), ()))

    def hidden(gate, up):
        left = lax.dot_general(values, gate[...], by_row, preferred_element_type=jnp.float32)
        right = lax.dot_general(values, up[...], by_row, preferred_element_type=jnp.float32)
        return (left / (1.0 + jnp.exp(-left)) * right).astype(jnp.bfloat16)

    hidden_a = hidden(gate_a, up_a)
    hidden_b = hidden(gate_b, up_b)
    width = held.shape[1] // PARTS
    copies = []
    for k in range(PARTS):
        span = pl.ds(k * width, width)
        total = dot(hidden_a, down_a[:, span]) + dot(hidden_b, down_b[:, span])
        held[:, span] = total.astype(jnp.bfloat16)
        copies.append(pltpu.make_async_copy(held.at[:, span], out.at[:, span], done.at[k]))
        copies[-1].start()
    for copy in copies:
        copy.wait()


def dot(left, right):
    return jnp.dot(left, right, preferred_element_type=jnp.float32)


def expert_half(
    shard,
    second_batch,
    expert_gain,
    expert_choice,
    route_scores,
    expert_gate,
    expert_up,
    expert_down,
):
    row_count, model_width = second_batch.shape
    experts = lax.axis_size(EP)
    capacity = 4 * row_count // experts
    half_slots = capacity // 2
    core = lax.axis_index("c")

    gate_own, up_own, down_own = expert_gate[0].T, expert_up[0].T, expert_down[0]
    gate_far = lax.ppermute(gate_own, "c", SWAP)
    up_far = lax.ppermute(up_own, "c", SWAP)
    down_far = lax.ppermute(down_own, "c", SWAP)

    normed = rms_scale(second_batch, expert_gain)
    expert_ids = jnp.arange(experts, dtype=jnp.int32)
    first_t = expert_choice[:, 0][None, :] == expert_ids[:, None]
    second_t = expert_choice[:, 1][None, :] == expert_ids[:, None]
    named_t = first_t | second_t
    rows = jnp.arange(row_count, dtype=jnp.int32)
    earlier_t = (rows[:, None] < rows[None, :]).astype(jnp.bfloat16)
    rank_t = dot(named_t.astype(jnp.bfloat16), earlier_t).astype(jnp.int32)
    rank_t = jnp.where(named_t, rank_t, -1)

    own_slots = core * half_slots + jnp.arange(half_slots, dtype=jnp.int32)
    spread = (rank_t[:, None, :] == own_slots[None, :, None]).astype(jnp.bfloat16)
    outgoing = dot(spread.reshape(experts * half_slots, row_count), normed).astype(jnp.bfloat16)
    outgoing = outgoing.reshape(experts, half_slots, model_width)
    shard, outgoing = lax.optimization_barrier((shard, outgoing))
    arrived = lax.all_to_all(outgoing, EP, 0, 0, tiled=True)
    incoming = arrived.reshape(experts * half_slots, model_width)

    partial = pl.pallas_call(
        ffn_body,
        out_shape=jax.ShapeDtypeStruct(incoming.shape, jnp.bfloat16),
        in_specs=[on_chip()] * 7,
        out_specs=pl.BlockSpec(memory_space=pltpu.HBM),
        scratch_shapes=[
            pltpu.VMEM(incoming.shape, jnp.bfloat16),
            pltpu.SemaphoreType.DMA((PARTS,)),
        ],
        compiler_params=pltpu.CompilerParams(vmem_limit_bytes=FFN_VMEM),
        cost_estimate=pl.CostEstimate(
            flops=12 * incoming.size * gate_own.shape[0],
            transcendentals=2 * incoming.shape[0] * gate_own.shape[0],
            bytes_accessed=4 * incoming.size + 12 * gate_own.size,
        ),
    )(incoming, gate_own, up_own, down_own, gate_far, up_far, down_far)
    shares = lax.axis_size(TP)
    piece = model_width // shares
    leaving = partial.reshape(experts, half_slots, shares, piece)
    leaving = jnp.moveaxis(leaving, 2, 1).reshape(experts * shares, half_slots, piece)
    returned = lax.all_to_all(leaving, ALL, 0, 0, tiled=True)
    returned = returned.reshape(experts, shares // 2, 2, half_slots, piece)
    results = jnp.sum(returned.astype(jnp.float32), axis=1).astype(jnp.bfloat16)
    results = results.reshape(experts * capacity, piece)

    weight_first = jax.nn.sigmoid(route_scores[:, 0] - route_scores[:, 1])[None, :]
    weight_t = jnp.where(first_t, weight_first, jnp.where(second_t, 1.0 - weight_first, 0.0))
    slots = jnp.arange(capacity, dtype=jnp.int32)
    blend_t = jnp.where(
        rank_t[:, None, :] == slots[None, :, None], weight_t[:, None, :], 0.0
    ).reshape(experts * capacity, row_count)
    high = lax.reduce_precision(blend_t, 8, 7)
    low = blend_t - high
    both = jnp.concatenate([high, low], axis=1).astype(jnp.bfloat16)
    mixed = lax.dot_general(
        both, results, (((0,), (0,)), ((), ())), preferred_element_type=jnp.float32
    )
    blended = (mixed[:row_count] + mixed[row_count:]).astype(jnp.bfloat16)

    whole = lax.all_gather(blended, TP)
    return jnp.transpose(whole, (1, 0, 2)).reshape(row_count, model_width), shard


def per_device(
    first_batch,
    mixer_gain,
    mixer_in,
    group_maps,
    pool_scale,
    mixer_out,
    second_batch,
    expert_gain,
    expert_choice,
    route_scores,
    expert_gate,
    expert_up,
    expert_down,
):
    shard = jnp.concatenate([mixer_in.T, mixer_out], axis=0)
    experts_second, shard = expert_half(
        shard,
        second_batch,
        expert_gain,
        expert_choice,
        route_scores,
        expert_gate,
        expert_up,
        expert_down,
    )
    mixed_first = mixer_half(first_batch, mixer_gain, shard, group_maps, pool_scale)
    return (mixed_first, experts_second)


def solution(mesh):
    torus = Mesh(mesh.devices.reshape(8, 4, mesh.shape["tp"] // 2, 2), ALL)
    placed = (
        P(ALL, None),
        P(),
        P(None, TP),
        P(),
        P(),
        P(TP, None),
        P(EP, None),
        P(),
        P(EP, None),
        P(EP, None),
        P(EP, None, TP),
        P(EP, None, TP),
        P(EP, TP, None),
    )
    return jax.shard_map(
        per_device,
        mesh=torus,
        in_specs=placed,
        out_specs=(P(ALL, None), P(EP, None)),
        check_vma=False,
    )
```

```python
import jax
import jax.numpy as jnp
from jax import lax
from jax.experimental import pallas as pl
from jax.experimental.pallas import tpu as pltpu
from jax.sharding import Mesh
from jax.sharding import PartitionSpec as P

GROUP = 64
ALL = ("z", "x", "y", "c")
EP = ("z", "x")
TP = ("y", "c")
PARTS = 4
EXPERTS = 32
SWAP = [(0, 1), (1, 0)]

epsilon = 1e-06


def neighbours(block, width):
    count = lax.axis_size(ALL)
    forward = [(i, i + 1) for i in range(count - 1)]
    backward = [(target, source) for source, target in forward]
    low = lax.ppermute(block[block.shape[0] - width :], ALL, forward)
    high = lax.ppermute(block[:width], ALL, backward)
    return low, high


def in_place():
    return pl.BlockSpec(memory_space=pl.ANY)


def in_scalars():
    return pl.BlockSpec(memory_space=pltpu.SMEM)


def limit(mib):
    return pltpu.CompilerParams(vmem_limit_bytes=mib << 20)


def norm(values, gain):
    floats = values.astype(jnp.float32)
    factor = lax.rsqrt(jnp.mean(floats * floats, axis=-1, keepdims=True) + epsilon)
    return (floats * factor * gain).astype(jnp.bfloat16)


def gathered_blocks(shard):
    size = lax.axis_size("y")
    far = lax.ppermute(shard, "c", SWAP)
    passed = jnp.concatenate([shard, far], axis=0)
    ways = [(2 * i, 2 * ((i + 1) % size)) for i in range(size)]
    ways += [(2 * i + 1, 2 * ((i - 1) % size) + 1) for i in range(size)]
    blocks = [passed]
    for _ in range(1, size // 2 + 1):
        passed = lax.ppermute(passed, TP, ways)
        blocks.append(passed)
    for step in range(1, size // 2):
        blocks.append(lax.ppermute(blocks[step], "c", SWAP))
    return blocks


def fetch(place, blocks, half, rows, done):
    size = len(blocks)
    share = rows.shape[0] // (2 * size)
    y, core = place[0], place[1]
    sign = 1 - 2 * core
    copies = []
    for k, block in enumerate(blocks):
        ours = k <= size // 2
        steps = -k if ours else k - size // 2
        group = lax.rem(y + sign * steps + size, size)
        first = core if ours else 1 - core
        for part in range(2):
            held = first if part == 0 else 1 - first
            start = pl.multiple_of((group * 2 + held) * share, share)
            base = (2 * part + half) * share
            copy = pltpu.make_async_copy(
                block.at[pl.ds(base, share), :],
                rows.at[pl.ds(start, share), :],
                done.at[2 * k + part],
            )
            copy.start()
            copies.append(copy)
    return copies


def project_body(place, rows, gain, *refs):
    blocks, pooled, in_rows, done = refs[:-3], refs[-3], refs[-2], refs[-1]
    copies = fetch(place, blocks, 0, in_rows, done)
    normed = norm(rows[...], gain[...])
    for copy in copies:
        copy.wait()
    product = lax.dot_general(
        normed, in_rows[...], (((1,), (1,)), ((), ())), preferred_element_type=jnp.float32
    )
    pooled[...] = product.astype(jnp.bfloat16)


def pool_body(place, pooled, low, high, maps, scale, *refs):
    blocks, out, out_rows, done = refs[:-3], refs[-3], refs[-2], refs[-1]
    copies = fetch(place, blocks, 1, out_rows, done)
    count_rows, channels = pooled.shape
    width = low.shape[0]
    pairs = maps.shape[0]
    lanes = maps.shape[1]
    middle = pooled[...].astype(jnp.float32)
    sums = jnp.concatenate(
        [low[...].astype(jnp.float32), middle, high[...].astype(jnp.float32)], axis=0
    )
    shape = (count_rows, channels)
    kind = lax.broadcasted_iota(jnp.int32, shape, 1) // GROUP % 4
    places = place[2] * count_rows + lax.broadcasted_iota(jnp.int32, shape, 0)
    length = place[3] * count_rows
    window_sum = jnp.zeros(shape, jnp.float32)
    for k in range(4):
        span = 1 << k
        kept = sums.shape[0] - span
        sums = sums[:kept] + sums[span:]
        window_sum = jnp.where(
            kind == k, sums[width - span : width - span + count_rows], window_sum
        )
    span = jnp.left_shift(jnp.ones(shape, jnp.int32), kind)
    window_count = jnp.minimum(places + span, length) - jnp.maximum(places - span, 0)
    centred = (window_sum / window_count.astype(jnp.float32) - middle).astype(jnp.bfloat16)
    pieces = []
    for k in range(pairs):
        lane = slice(k * lanes, (k + 1) * lanes)
        pieces.append((dot(centred[:, lane], maps[k]) * scale[:, lane]).astype(jnp.bfloat16))
    grouped = jnp.concatenate(pieces, axis=1)
    for copy in copies:
        copy.wait()
    out[...] = dot(grouped, out_rows[...]).astype(jnp.bfloat16)


def mixer_half(first_batch, mixer_gain, shard, pair_maps, pool_scale):
    count_rows, width = first_batch.shape
    channels = pool_scale.shape[0]
    blocks = gathered_blocks(shard)
    place = jnp.stack(
        [
            lax.axis_index("y"),
            lax.axis_index("c"),
            lax.axis_index(ALL),
            jnp.int32(lax.axis_size(ALL)),
        ]
    ).astype(jnp.int32)
    held = [
        pltpu.VMEM((channels, width), jnp.bfloat16),
        pltpu.SemaphoreType.DMA((2 * len(blocks),)),
    ]
    cost = pl.CostEstimate(
        flops=2 * count_rows * width * channels,
        transcendentals=0,
        bytes_accessed=4 * channels * width,
    )
    whole = pl.BlockSpec()
    pooled_in = pl.pallas_call(
        project_body,
        out_shape=jax.ShapeDtypeStruct((count_rows, channels), jnp.bfloat16),
        in_specs=[in_scalars(), whole, whole] + [in_place()] * len(blocks),
        scratch_shapes=held,
        compiler_params=limit(10),
        cost_estimate=cost,
    )(place, first_batch, mixer_gain[None, :], *blocks)
    low, high = neighbours(pooled_in, 8)
    return pl.pallas_call(
        pool_body,
        out_shape=jax.ShapeDtypeStruct((count_rows, width), jnp.bfloat16),
        in_specs=[in_scalars()] + [whole] * 5 + [in_place()] * len(blocks),
        scratch_shapes=held,
        compiler_params=limit(10),
        cost_estimate=cost,
    )(place, pooled_in, low, high, pair_maps, pool_scale[None, :], *blocks)


def ranked(choice, experts):
    count = choice.shape[1]
    names = lax.broadcasted_iota(jnp.int32, (experts, count), 0)
    first = choice[0:1, :] == names
    second = choice[1:2, :] == names
    named = first | second
    rows = lax.broadcasted_iota(jnp.int32, (count, count), 0)
    others = lax.broadcasted_iota(jnp.int32, (count, count), 1)
    earlier = jnp.where(rows < others, 1.0, 0.0).astype(jnp.bfloat16)
    rank = dot(jnp.where(named, 1.0, 0.0).astype(jnp.bfloat16), earlier)
    return first, second, jnp.where(named, rank, -1.0).astype(jnp.bfloat16)


def repeated(values, repeats):
    experts = values.shape[0]
    shape = (experts * repeats, experts)
    owner = lax.broadcasted_iota(jnp.int32, shape, 0) // repeats
    match = owner == lax.broadcasted_iota(jnp.int32, shape, 1)
    return dot(jnp.where(match, 1.0, 0.0).astype(jnp.bfloat16), values)


def dispatch_body(core, rows, gain, choice, out):
    count = rows.shape[0]
    slots = out.shape[0]
    half = slots // EXPERTS
    rank = repeated(ranked(choice[...], EXPERTS)[2], half)
    slot = core[0] * half + lax.broadcasted_iota(jnp.int32, (slots, count), 0) % half
    spread = jnp.where(rank == slot.astype(jnp.float32), 1.0, 0.0).astype(jnp.bfloat16)
    out[...] = dot(spread, norm(rows[...], gain[...])).astype(jnp.bfloat16)


def blend_body(choice, scores, out):
    count = choice.shape[1]
    slots = out.shape[0]
    first, second, rank = ranked(choice[...], EXPERTS)
    repeats = slots // EXPERTS
    weight = 1.0 / (1.0 + jnp.exp(scores[1:2, :] - scores[0:1, :]))
    weights = jnp.where(first, weight, jnp.where(second, 1.0 - weight, 0.0))
    high = weights.astype(jnp.bfloat16)
    low = (weights - high.astype(jnp.float32)).astype(jnp.bfloat16)
    slot = lax.broadcasted_iota(jnp.int32, (slots, count), 0) % repeats
    match = repeated(rank, repeats) == slot.astype(jnp.float32)
    out[:, :count] = jnp.where(match, repeated(high, repeats), 0.0).astype(jnp.bfloat16)
    out[:, count:] = jnp.where(match, repeated(low, repeats), 0.0).astype(jnp.bfloat16)


def ffn_body(*refs):
    sources, out, held, done = refs[:7], refs[7], refs[8:16], refs[16]
    fetches = []
    for k in range(7):
        fetches.append(pltpu.make_async_copy(sources[k], held[k], done.at[PARTS + k]))
        fetches[-1].start()
    rows, _, _, down_a, _, _, down_b, result = held
    fetches[0].wait()
    values = rows[...]

    def product(k):
        fetches[k].wait()
        return lax.dot_general(
            values, held[k][...], (((1,), (1,)), ((), ())), preferred_element_type=jnp.float32
        )

    def hidden(gate, up):
        return (gate / (1.0 + jnp.exp(-gate)) * up).astype(jnp.bfloat16)

    hidden_a = hidden(product(1), product(2))
    hidden_b = hidden(product(4), product(5))
    fetches[3].wait()
    fetches[6].wait()
    width = result.shape[1] // PARTS
    copies = []
    for k in range(PARTS):
        span = pl.ds(k * width, width)
        total = dot(hidden_a, down_a[:, span]) + dot(hidden_b, down_b[:, span])
        result[:, span] = total.astype(jnp.bfloat16)
        copies.append(pltpu.make_async_copy(result.at[:, span], out.at[:, span], done.at[k]))
        copies[-1].start()
    for copy in copies:
        copy.wait()


def dot(left, right):
    return jnp.dot(left, right, preferred_element_type=jnp.float32)


def expert_half(
    mixer_in,
    mixer_out,
    second_batch,
    expert_gain,
    expert_choice,
    route_scores,
    expert_gate,
    expert_up,
    expert_down,
):
    row_count, model_width = second_batch.shape
    experts = lax.axis_size(EP)
    capacity = 4 * row_count // experts
    half_slots = capacity // 2
    core = lax.axis_index("c")

    gate_own, up_own, down_own = expert_gate[0].T, expert_up[0].T, expert_down[0]
    gate_far = lax.ppermute(gate_own, "c", SWAP)
    up_far = lax.ppermute(up_own, "c", SWAP)
    down_far = lax.ppermute(down_own, "c", SWAP)

    outgoing = pl.pallas_call(
        dispatch_body,
        out_shape=jax.ShapeDtypeStruct((experts * half_slots, model_width), jnp.bfloat16),
        in_specs=[in_scalars()] + [pl.BlockSpec()] * 3,
        compiler_params=limit(8),
        cost_estimate=pl.CostEstimate(
            flops=2 * experts * half_slots * second_batch.size,
            transcendentals=row_count,
            bytes_accessed=6 * second_batch.size,
        ),
    )(core[None].astype(jnp.int32), second_batch, expert_gain[None, :], expert_choice.T)
    outgoing = outgoing.reshape(experts, half_slots, model_width)
    mixer_in, mixer_out, outgoing = lax.optimization_barrier((mixer_in, mixer_out, outgoing))
    shard = jnp.concatenate([mixer_in.T, mixer_out], axis=0)
    arrived = lax.all_to_all(outgoing, EP, 0, 0, tiled=True)
    incoming = arrived.reshape(experts * half_slots, model_width)

    partial = pl.pallas_call(
        ffn_body,
        out_shape=jax.ShapeDtypeStruct(incoming.shape, jnp.bfloat16),
        in_specs=[in_place()] * 7,
        out_specs=in_place(),
        scratch_shapes=[pltpu.VMEM(incoming.shape, jnp.bfloat16)]
        + [pltpu.VMEM(gate_own.shape, jnp.bfloat16)] * 6
        + [pltpu.VMEM(incoming.shape, jnp.bfloat16), pltpu.SemaphoreType.DMA((PARTS + 7,))],
        compiler_params=limit(14),
        cost_estimate=pl.CostEstimate(
            flops=12 * incoming.size * gate_own.shape[0],
            transcendentals=2 * incoming.shape[0] * gate_own.shape[0],
            bytes_accessed=4 * incoming.size + 12 * gate_own.size,
        ),
    )(incoming, gate_own, up_own, down_own, gate_far, up_far, down_far)
    shares = lax.axis_size(TP)
    piece = model_width // shares
    leaving = partial.reshape(experts, half_slots, shares, piece)
    leaving = jnp.moveaxis(leaving, 2, 1).reshape(experts * shares, half_slots, piece)
    returned = lax.all_to_all(leaving, ALL, 0, 0, tiled=True)
    returned = returned.reshape(experts, shares // 2, 2, half_slots, piece)
    results = jnp.sum(returned.astype(jnp.float32), axis=1).astype(jnp.bfloat16)
    results = results.reshape(experts * capacity, piece)

    both = pl.pallas_call(
        blend_body,
        out_shape=jax.ShapeDtypeStruct((experts * capacity, 2 * row_count), jnp.bfloat16),
        compiler_params=limit(6),
    )(expert_choice.T, route_scores.T)
    mixed = lax.dot_general(
        both, results, (((0,), (0,)), ((), ())), preferred_element_type=jnp.float32
    )
    blended = (mixed[:row_count] + mixed[row_count:]).astype(jnp.bfloat16)

    whole = lax.all_gather(blended, TP)
    return jnp.transpose(whole, (1, 0, 2)).reshape(row_count, model_width), shard


def per_device(
    first_batch,
    mixer_gain,
    mixer_in,
    group_maps,
    pool_scale,
    mixer_out,
    second_batch,
    expert_gain,
    expert_choice,
    route_scores,
    expert_gate,
    expert_up,
    expert_down,
):
    experts_second, shard = expert_half(
        mixer_in,
        mixer_out,
        second_batch,
        expert_gain,
        expert_choice,
        route_scores,
        expert_gate,
        expert_up,
        expert_down,
    )
    groups, inner, outer = group_maps.shape
    same = jnp.eye(2, dtype=jnp.bfloat16)
    pair_maps = jnp.einsum("pgcd,gh->pgchd", group_maps.reshape(groups // 2, 2, inner, outer), same)
    pair_maps = pair_maps.reshape(groups // 2, 2 * inner, 2 * outer)
    mixed_first = mixer_half(first_batch, mixer_gain, shard, pair_maps, pool_scale)
    return (mixed_first, experts_second)


def solution(mesh):
    torus = Mesh(mesh.devices.reshape(8, 4, mesh.shape["tp"] // 2, 2), ALL)
    placed = (
        P(ALL, None),
        P(),
        P(None, TP),
        P(),
        P(),
        P(TP, None),
        P(EP, None),
        P(),
        P(EP, None),
        P(EP, None),
        P(EP, None, TP),
        P(EP, None, TP),
        P(EP, TP, None),
    )
    return jax.shard_map(
        per_device,
        mesh=torus,
        in_specs=placed,
        out_specs=(P(ALL, None), P(EP, None)),
        check_vma=False,
    )
```

```python
import jax
import jax.numpy as jnp
from jax import lax
from jax.experimental import pallas as pl
from jax.experimental.pallas import tpu as pltpu
from jax.sharding import Mesh
from jax.sharding import PartitionSpec as P

GROUP = 64
ALL = ("z", "x", "y", "c")
EP = ("z", "x")
TP = ("y", "c")
PARTS = 4
EXPERTS = 32
SWAP = [(0, 1), (1, 0)]

epsilon = 1e-06


def neighbours(block, width):
    count = lax.axis_size(ALL)
    forward = [(i, i + 1) for i in range(count - 1)]
    backward = [(target, source) for source, target in forward]
    low = lax.ppermute(block[block.shape[0] - width :], ALL, forward)
    high = lax.ppermute(block[:width], ALL, backward)
    return low, high


def in_place():
    return pl.BlockSpec(memory_space=pl.ANY)


def in_scalars():
    return pl.BlockSpec(memory_space=pltpu.SMEM)


def limit(mib):
    return pltpu.CompilerParams(vmem_limit_bytes=mib << 20)


def norm(values, gain):
    floats = values.astype(jnp.float32)
    factor = lax.rsqrt(jnp.mean(floats * floats, axis=-1, keepdims=True) + epsilon)
    return (floats * factor * gain).astype(jnp.bfloat16)


def fetch(blocks, half, rows, done):
    share = blocks.shape[1] // 2
    copies = []
    for k in range(blocks.shape[0]):
        copy = pltpu.make_async_copy(
            blocks.at[k, pl.ds(half * share, share), :],
            rows.at[pl.ds(k * share, share), :],
            done.at[k],
        )
        copy.start()
        copies.append(copy)
    return copies


def project_body(rows, gain, blocks, pooled, in_rows, done):
    copies = fetch(blocks, 0, in_rows, done)
    normed = norm(rows[...], gain[...])
    for copy in copies:
        copy.wait()
    product = lax.dot_general(
        normed, in_rows[...], (((1,), (1,)), ((), ())), preferred_element_type=jnp.float32
    )
    pooled[...] = product.astype(jnp.bfloat16)


def pool_body(place, pooled, low, high, maps, scale, blocks, out, out_rows, done):
    copies = fetch(blocks, 1, out_rows, done)
    count_rows, channels = pooled.shape
    width = low.shape[0]
    pairs = maps.shape[0]
    lanes = maps.shape[1]
    middle = pooled[...].astype(jnp.float32)
    sums = jnp.concatenate(
        [low[...].astype(jnp.float32), middle, high[...].astype(jnp.float32)], axis=0
    )
    shape = (count_rows, channels)
    kind = lax.broadcasted_iota(jnp.int32, shape, 1) // GROUP % 4
    places = place[0] * count_rows + lax.broadcasted_iota(jnp.int32, shape, 0)
    length = place[1] * count_rows
    window_sum = jnp.zeros(shape, jnp.float32)
    for k in range(4):
        span = 1 << k
        kept = sums.shape[0] - span
        sums = sums[:kept] + sums[span:]
        window_sum = jnp.where(
            kind == k, sums[width - span : width - span + count_rows], window_sum
        )
    span = jnp.left_shift(jnp.ones(shape, jnp.int32), kind)
    window_count = jnp.minimum(places + span, length) - jnp.maximum(places - span, 0)
    centred = (window_sum / window_count.astype(jnp.float32) - middle).astype(jnp.bfloat16)
    pieces = []
    for k in range(pairs):
        lane = slice(k * lanes, (k + 1) * lanes)
        pieces.append((dot(centred[:, lane], maps[k]) * scale[:, lane]).astype(jnp.bfloat16))
    grouped = jnp.concatenate(pieces, axis=1)
    for copy in copies:
        copy.wait()
    out[...] = dot(grouped, out_rows[...]).astype(jnp.bfloat16)


def mixer_half(first_batch, mixer_gain, shard, pair_maps, pool_scale):
    count_rows, width = first_batch.shape
    channels = pool_scale.shape[0]
    blocks = lax.all_gather(shard, TP)
    place = jnp.stack([lax.axis_index(ALL), jnp.int32(lax.axis_size(ALL))]).astype(jnp.int32)
    held = [
        pltpu.VMEM((channels, width), jnp.bfloat16),
        pltpu.SemaphoreType.DMA((blocks.shape[0],)),
    ]
    cost = pl.CostEstimate(
        flops=2 * count_rows * width * channels,
        transcendentals=0,
        bytes_accessed=4 * channels * width,
    )
    whole = pl.BlockSpec()
    pooled_in = pl.pallas_call(
        project_body,
        out_shape=jax.ShapeDtypeStruct((count_rows, channels), jnp.bfloat16),
        in_specs=[whole, whole, in_place()],
        scratch_shapes=held,
        compiler_params=limit(59),
        cost_estimate=cost,
    )(first_batch, mixer_gain[None, :], blocks)
    low, high = neighbours(pooled_in, 8)
    return pl.pallas_call(
        pool_body,
        out_shape=jax.ShapeDtypeStruct((count_rows, width), jnp.bfloat16),
        in_specs=[in_scalars()] + [whole] * 5 + [in_place()],
        scratch_shapes=held,
        compiler_params=limit(59),
        cost_estimate=cost,
    )(place, pooled_in, low, high, pair_maps, pool_scale[None, :], blocks)


def ranked(choice, experts):
    count = choice.shape[1]
    names = lax.broadcasted_iota(jnp.int32, (experts, count), 0)
    first = choice[0:1, :] == names
    second = choice[1:2, :] == names
    named = first | second
    rows = lax.broadcasted_iota(jnp.int32, (count, count), 0)
    others = lax.broadcasted_iota(jnp.int32, (count, count), 1)
    earlier = jnp.where(rows < others, 1.0, 0.0).astype(jnp.bfloat16)
    rank = dot(jnp.where(named, 1.0, 0.0).astype(jnp.bfloat16), earlier)
    return first, second, jnp.where(named, rank, -1.0).astype(jnp.bfloat16)


def repeated(values, repeats):
    experts = values.shape[0]
    shape = (experts * repeats, experts)
    owner = lax.broadcasted_iota(jnp.int32, shape, 0) // repeats
    match = owner == lax.broadcasted_iota(jnp.int32, shape, 1)
    return dot(jnp.where(match, 1.0, 0.0).astype(jnp.bfloat16), values)


def dispatch_body(core, rows, gain, choice, out):
    count = rows.shape[0]
    slots = out.shape[0]
    half = slots // EXPERTS
    rank = repeated(ranked(choice[...], EXPERTS)[2], half)
    slot = core[0] * half + lax.broadcasted_iota(jnp.int32, (slots, count), 0) % half
    spread = jnp.where(rank == slot.astype(jnp.float32), 1.0, 0.0).astype(jnp.bfloat16)
    out[...] = dot(spread, norm(rows[...], gain[...])).astype(jnp.bfloat16)


def blend_body(choice, scores, out):
    count = choice.shape[1]
    slots = out.shape[0]
    first, second, rank = ranked(choice[...], EXPERTS)
    repeats = slots // EXPERTS
    weight = 1.0 / (1.0 + jnp.exp(scores[1:2, :] - scores[0:1, :]))
    weights = jnp.where(first, weight, jnp.where(second, 1.0 - weight, 0.0))
    high = weights.astype(jnp.bfloat16)
    low = (weights - high.astype(jnp.float32)).astype(jnp.bfloat16)
    slot = lax.broadcasted_iota(jnp.int32, (slots, count), 0) % repeats
    match = repeated(rank, repeats) == slot.astype(jnp.float32)
    out[:, :count] = jnp.where(match, repeated(high, repeats), 0.0).astype(jnp.bfloat16)
    out[:, count:] = jnp.where(match, repeated(low, repeats), 0.0).astype(jnp.bfloat16)


def ffn_body(*refs):
    sources, out, held, done = refs[:7], refs[7], refs[8:16], refs[16]
    fetches = []
    for k in range(7):
        fetches.append(pltpu.make_async_copy(sources[k], held[k], done.at[PARTS + k]))
        fetches[-1].start()
    rows, _, _, down_a, _, _, down_b, result = held
    fetches[0].wait()
    values = rows[...]

    def product(k):
        fetches[k].wait()
        return lax.dot_general(
            values, held[k][...], (((1,), (1,)), ((), ())), preferred_element_type=jnp.float32
        )

    def hidden(gate, up):
        return (gate / (1.0 + jnp.exp(-gate)) * up).astype(jnp.bfloat16)

    hidden_a = hidden(product(1), product(2))
    hidden_b = hidden(product(4), product(5))
    fetches[3].wait()
    fetches[6].wait()
    width = result.shape[1] // PARTS
    copies = []
    for k in range(PARTS):
        span = pl.ds(k * width, width)
        total = dot(hidden_a, down_a[:, span]) + dot(hidden_b, down_b[:, span])
        result[:, span] = total.astype(jnp.bfloat16)
        copies.append(pltpu.make_async_copy(result.at[:, span], out.at[:, span], done.at[k]))
        copies[-1].start()
    for copy in copies:
        copy.wait()


def dot(left, right):
    return jnp.dot(left, right, preferred_element_type=jnp.float32)


def expert_half(
    mixer_in,
    mixer_out,
    second_batch,
    expert_gain,
    expert_choice,
    route_scores,
    expert_gate,
    expert_up,
    expert_down,
):
    row_count, model_width = second_batch.shape
    experts = lax.axis_size(EP)
    capacity = 4 * row_count // experts
    half_slots = capacity // 2
    core = lax.axis_index("c")

    gate_own, up_own, down_own = expert_gate[0].T, expert_up[0].T, expert_down[0]
    gate_far = lax.ppermute(gate_own, "c", SWAP)
    up_far = lax.ppermute(up_own, "c", SWAP)
    down_far = lax.ppermute(down_own, "c", SWAP)

    outgoing = pl.pallas_call(
        dispatch_body,
        out_shape=jax.ShapeDtypeStruct((experts * half_slots, model_width), jnp.bfloat16),
        in_specs=[in_scalars()] + [pl.BlockSpec()] * 3,
        compiler_params=limit(8),
        cost_estimate=pl.CostEstimate(
            flops=2 * experts * half_slots * second_batch.size,
            transcendentals=row_count,
            bytes_accessed=6 * second_batch.size,
        ),
    )(core[None].astype(jnp.int32), second_batch, expert_gain[None, :], expert_choice.T)
    outgoing = outgoing.reshape(experts, half_slots, model_width)
    mixer_in, mixer_out, outgoing = lax.optimization_barrier((mixer_in, mixer_out, outgoing))
    shard = jnp.concatenate([mixer_in.T, mixer_out], axis=0)
    arrived = lax.all_to_all(outgoing, EP, 0, 0, tiled=True)
    incoming = arrived.reshape(experts * half_slots, model_width)

    partial = pl.pallas_call(
        ffn_body,
        out_shape=jax.ShapeDtypeStruct(incoming.shape, jnp.bfloat16),
        in_specs=[in_place()] * 7,
        out_specs=in_place(),
        scratch_shapes=[pltpu.VMEM(incoming.shape, jnp.bfloat16)]
        + [pltpu.VMEM(gate_own.shape, jnp.bfloat16)] * 6
        + [pltpu.VMEM(incoming.shape, jnp.bfloat16), pltpu.SemaphoreType.DMA((PARTS + 7,))],
        compiler_params=limit(60),
        cost_estimate=pl.CostEstimate(
            flops=12 * incoming.size * gate_own.shape[0],
            transcendentals=2 * incoming.shape[0] * gate_own.shape[0],
            bytes_accessed=4 * incoming.size + 12 * gate_own.size,
        ),
    )(incoming, gate_own, up_own, down_own, gate_far, up_far, down_far)
    shares = lax.axis_size(TP)
    piece = model_width // shares
    leaving = partial.reshape(experts, half_slots, shares, piece)
    leaving = jnp.moveaxis(leaving, 2, 1).reshape(experts * shares, half_slots, piece)
    returned = lax.all_to_all(leaving, ALL, 0, 0, tiled=True)
    returned = returned.reshape(experts, shares // 2, 2, half_slots, piece)
    results = jnp.sum(returned.astype(jnp.float32), axis=1).astype(jnp.bfloat16)
    results = results.reshape(experts * capacity, piece)

    both = pl.pallas_call(
        blend_body,
        out_shape=jax.ShapeDtypeStruct((experts * capacity, 2 * row_count), jnp.bfloat16),
        compiler_params=limit(6),
    )(expert_choice.T, route_scores.T)
    mixed = lax.dot_general(
        both, results, (((0,), (0,)), ((), ())), preferred_element_type=jnp.float32
    )
    blended = (mixed[:row_count] + mixed[row_count:]).astype(jnp.bfloat16)

    whole = lax.all_gather(blended, TP)
    return jnp.transpose(whole, (1, 0, 2)).reshape(row_count, model_width), shard


def per_device(
    first_batch,
    mixer_gain,
    mixer_in,
    group_maps,
    pool_scale,
    mixer_out,
    second_batch,
    expert_gain,
    expert_choice,
    route_scores,
    expert_gate,
    expert_up,
    expert_down,
):
    experts_second, shard = expert_half(
        mixer_in,
        mixer_out,
        second_batch,
        expert_gain,
        expert_choice,
        route_scores,
        expert_gate,
        expert_up,
        expert_down,
    )
    groups, inner, outer = group_maps.shape
    same = jnp.eye(2, dtype=jnp.bfloat16)
    pair_maps = jnp.einsum("pgcd,gh->pgchd", group_maps.reshape(groups // 2, 2, inner, outer), same)
    pair_maps = pair_maps.reshape(groups // 2, 2 * inner, 2 * outer)
    mixed_first = mixer_half(first_batch, mixer_gain, shard, pair_maps, pool_scale)
    return (mixed_first, experts_second)


def solution(mesh):
    torus = Mesh(mesh.devices.reshape(8, 4, mesh.shape["tp"] // 2, 2), ALL)
    placed = (
        P(ALL, None),
        P(),
        P(None, TP),
        P(),
        P(),
        P(TP, None),
        P(EP, None),
        P(),
        P(EP, None),
        P(EP, None),
        P(EP, None, TP),
        P(EP, None, TP),
        P(EP, TP, None),
    )
    return jax.shard_map(
        per_device,
        mesh=torus,
        in_specs=placed,
        out_specs=(P(ALL, None), P(EP, None)),
        check_vma=False,
    )
```

```python
import jax
import jax.numpy as jnp
from jax import lax
from jax.experimental import pallas as pl
from jax.experimental.pallas import tpu as pltpu
from jax.sharding import Mesh
from jax.sharding import PartitionSpec as P

GROUP = 64
ALL = ("z", "x", "y", "c")
EP = ("z", "x")
TP = ("y", "c")
PARTS = 4
EXPERTS = 32
SWAP = [(0, 1), (1, 0)]

epsilon = 1e-06


def neighbours(block, width):
    count = lax.axis_size(ALL)
    forward = [(i, i + 1) for i in range(count - 1)]
    backward = [(target, source) for source, target in forward]
    low = lax.ppermute(block[block.shape[0] - width :], ALL, forward)
    high = lax.ppermute(block[:width], ALL, backward)
    return low, high


def in_place():
    return pl.BlockSpec(memory_space=pl.ANY)


def in_scalars():
    return pl.BlockSpec(memory_space=pltpu.SMEM)


def limit(mib):
    return pltpu.CompilerParams(vmem_limit_bytes=mib << 20)


def norm(values, gain):
    floats = values.astype(jnp.float32)
    factor = lax.rsqrt(jnp.mean(floats * floats, axis=-1, keepdims=True) + epsilon)
    return (floats * factor * gain).astype(jnp.bfloat16)


def fetch(blocks, half, rows, done):
    share = blocks.shape[1] // 2
    copies = []
    for k in range(blocks.shape[0]):
        copy = pltpu.make_async_copy(
            blocks.at[k, pl.ds(half * share, share), :],
            rows.at[pl.ds(k * share, share), :],
            done.at[k],
        )
        copy.start()
        copies.append(copy)
    return copies


def project_body(rows, gain, blocks, pooled, in_rows, done):
    copies = fetch(blocks, 0, in_rows, done)
    normed = norm(rows[...], gain[...])
    for copy in copies:
        copy.wait()
    product = lax.dot_general(
        normed, in_rows[...], (((1,), (1,)), ((), ())), preferred_element_type=jnp.float32
    )
    pooled[...] = product.astype(jnp.bfloat16)


def pool_body(place, pooled, low, high, maps, scale, blocks, out, out_rows, done):
    copies = fetch(blocks, 1, out_rows, done)
    count_rows, channels = pooled.shape
    width = low.shape[0]
    pairs = maps.shape[0]
    lanes = maps.shape[1]
    middle = pooled[...].astype(jnp.float32)
    sums = jnp.concatenate(
        [low[...].astype(jnp.float32), middle, high[...].astype(jnp.float32)], axis=0
    )
    shape = (count_rows, channels)
    kind = lax.broadcasted_iota(jnp.int32, shape, 1) // GROUP % 4
    places = place[0] * count_rows + lax.broadcasted_iota(jnp.int32, shape, 0)
    length = place[1] * count_rows
    window_sum = jnp.zeros(shape, jnp.float32)
    for k in range(4):
        span = 1 << k
        kept = sums.shape[0] - span
        sums = sums[:kept] + sums[span:]
        window_sum = jnp.where(
            kind == k, sums[width - span : width - span + count_rows], window_sum
        )
    span = jnp.left_shift(jnp.ones(shape, jnp.int32), kind)
    window_count = jnp.minimum(places + span, length) - jnp.maximum(places - span, 0)
    centred = (window_sum / window_count.astype(jnp.float32) - middle).astype(jnp.bfloat16)
    pieces = []
    for k in range(pairs):
        lane = slice(k * lanes, (k + 1) * lanes)
        pieces.append((dot(centred[:, lane], maps[k]) * scale[:, lane]).astype(jnp.bfloat16))
    grouped = jnp.concatenate(pieces, axis=1)
    for copy in copies:
        copy.wait()
    out[...] = dot(grouped, out_rows[...]).astype(jnp.bfloat16)


def mixer_half(first_batch, mixer_gain, shard, pair_maps, pool_scale):
    count_rows, width = first_batch.shape
    channels = pool_scale.shape[0]
    blocks = lax.all_gather(shard, TP)
    place = jnp.stack([lax.axis_index(ALL), jnp.int32(lax.axis_size(ALL))]).astype(jnp.int32)
    held = [
        pltpu.VMEM((channels, width), jnp.bfloat16),
        pltpu.SemaphoreType.DMA((blocks.shape[0],)),
    ]
    cost = pl.CostEstimate(
        flops=2 * count_rows * width * channels,
        transcendentals=0,
        bytes_accessed=4 * channels * width,
    )
    whole = pl.BlockSpec()
    pooled_in = pl.pallas_call(
        project_body,
        out_shape=jax.ShapeDtypeStruct((count_rows, channels), jnp.bfloat16),
        in_specs=[whole, whole, in_place()],
        scratch_shapes=held,
        compiler_params=limit(59),
        cost_estimate=cost,
    )(first_batch, mixer_gain[None, :], blocks)
    low, high = neighbours(pooled_in, 8)
    return pl.pallas_call(
        pool_body,
        out_shape=jax.ShapeDtypeStruct((count_rows, width), jnp.bfloat16),
        in_specs=[in_scalars()] + [whole] * 5 + [in_place()],
        scratch_shapes=held,
        compiler_params=limit(59),
        cost_estimate=cost,
    )(place, pooled_in, low, high, pair_maps, pool_scale[None, :], blocks)


def ranked(choice, experts):
    count = choice.shape[1]
    names = lax.broadcasted_iota(jnp.int32, (experts, count), 0)
    first = choice[0:1, :] == names
    second = choice[1:2, :] == names
    named = first | second
    rows = lax.broadcasted_iota(jnp.int32, (count, count), 0)
    others = lax.broadcasted_iota(jnp.int32, (count, count), 1)
    earlier = jnp.where(rows < others, 1.0, 0.0).astype(jnp.bfloat16)
    rank = dot(jnp.where(named, 1.0, 0.0).astype(jnp.bfloat16), earlier)
    return first, second, jnp.where(named, rank, -1.0).astype(jnp.bfloat16)


def repeated(values, repeats):
    experts = values.shape[0]
    shape = (experts * repeats, experts)
    owner = lax.broadcasted_iota(jnp.int32, shape, 0) // repeats
    match = owner == lax.broadcasted_iota(jnp.int32, shape, 1)
    return dot(jnp.where(match, 1.0, 0.0).astype(jnp.bfloat16), values)


def dispatch_body(core, rows_from, gain_from, choice_from, out, rows, gain, choice, done):
    copies = []
    for k, (source, held) in enumerate(
        ((choice_from, choice), (rows_from, rows), (gain_from, gain))
    ):
        copies.append(pltpu.make_async_copy(source, held, done.at[k]))
        copies[-1].start()
    count = rows.shape[0]
    slots = out.shape[0]
    half = slots // EXPERTS
    slot = core[0] * half + lax.broadcasted_iota(jnp.int32, (slots, count), 0) % half
    copies[0].wait()
    rank = repeated(ranked(choice[...], EXPERTS)[2], half)
    spread = jnp.where(rank == slot.astype(jnp.float32), 1.0, 0.0).astype(jnp.bfloat16)
    copies[1].wait()
    copies[2].wait()
    out[...] = dot(spread, norm(rows[...], gain[...])).astype(jnp.bfloat16)


def blend_body(choice, scores, out):
    count = choice.shape[1]
    slots = out.shape[0]
    first, second, rank = ranked(choice[...], EXPERTS)
    repeats = slots // EXPERTS
    weight = 1.0 / (1.0 + jnp.exp(scores[1:2, :] - scores[0:1, :]))
    weights = jnp.where(first, weight, jnp.where(second, 1.0 - weight, 0.0))
    high = weights.astype(jnp.bfloat16)
    low = (weights - high.astype(jnp.float32)).astype(jnp.bfloat16)
    slot = lax.broadcasted_iota(jnp.int32, (slots, count), 0) % repeats
    match = repeated(rank, repeats) == slot.astype(jnp.float32)
    out[:, :count] = jnp.where(match, repeated(high, repeats), 0.0).astype(jnp.bfloat16)
    out[:, count:] = jnp.where(match, repeated(low, repeats), 0.0).astype(jnp.bfloat16)


def ffn_body(*refs):
    sources, out, held, done = refs[:7], refs[7], refs[8:16], refs[16]
    fetches = []
    for k in range(7):
        fetches.append(pltpu.make_async_copy(sources[k], held[k], done.at[PARTS + k]))
        fetches[-1].start()
    rows, _, _, down_a, _, _, down_b, result = held
    fetches[0].wait()
    values = rows[...]

    def product(k):
        fetches[k].wait()
        return lax.dot_general(
            values, held[k][...], (((1,), (1,)), ((), ())), preferred_element_type=jnp.float32
        )

    def hidden(gate, up):
        return (gate / (1.0 + jnp.exp(-gate)) * up).astype(jnp.bfloat16)

    hidden_a = hidden(product(1), product(2))
    hidden_b = hidden(product(4), product(5))
    fetches[3].wait()
    fetches[6].wait()
    width = result.shape[1] // PARTS
    copies = []
    for k in range(PARTS):
        span = pl.ds(k * width, width)
        total = dot(hidden_a, down_a[:, span]) + dot(hidden_b, down_b[:, span])
        result[:, span] = total.astype(jnp.bfloat16)
        copies.append(pltpu.make_async_copy(result.at[:, span], out.at[:, span], done.at[k]))
        copies[-1].start()
    for copy in copies:
        copy.wait()


def dot(left, right):
    return jnp.dot(left, right, preferred_element_type=jnp.float32)


def expert_half(
    mixer_in,
    mixer_out,
    second_batch,
    expert_gain,
    expert_choice,
    route_scores,
    expert_gate,
    expert_up,
    expert_down,
):
    row_count, model_width = second_batch.shape
    experts = lax.axis_size(EP)
    capacity = 4 * row_count // experts
    half_slots = capacity // 2
    core = lax.axis_index("c")

    gate_own, up_own, down_own = expert_gate[0].T, expert_up[0].T, expert_down[0]
    gate_far = lax.ppermute(gate_own, "c", SWAP)
    up_far = lax.ppermute(up_own, "c", SWAP)
    down_far = lax.ppermute(down_own, "c", SWAP)

    outgoing = pl.pallas_call(
        dispatch_body,
        out_shape=jax.ShapeDtypeStruct((experts * half_slots, model_width), jnp.bfloat16),
        in_specs=[in_scalars()] + [in_place()] * 3,
        scratch_shapes=[
            pltpu.VMEM(second_batch.shape, second_batch.dtype),
            pltpu.VMEM((1, model_width), jnp.float32),
            pltpu.VMEM((expert_choice.shape[1], row_count), jnp.int32),
            pltpu.SemaphoreType.DMA((3,)),
        ],
        compiler_params=limit(61),
        cost_estimate=pl.CostEstimate(
            flops=2 * experts * half_slots * second_batch.size,
            transcendentals=row_count,
            bytes_accessed=6 * second_batch.size,
        ),
    )(core[None].astype(jnp.int32), second_batch, expert_gain[None, :], expert_choice.T)
    outgoing = outgoing.reshape(experts, half_slots, model_width)
    mixer_in, mixer_out, outgoing = lax.optimization_barrier((mixer_in, mixer_out, outgoing))
    shard = jnp.concatenate([mixer_in.T, mixer_out], axis=0)
    arrived = lax.all_to_all(outgoing, EP, 0, 0, tiled=True)
    incoming = arrived.reshape(experts * half_slots, model_width)

    partial = pl.pallas_call(
        ffn_body,
        out_shape=jax.ShapeDtypeStruct(incoming.shape, jnp.bfloat16),
        in_specs=[in_place()] * 7,
        out_specs=in_place(),
        scratch_shapes=[pltpu.VMEM(incoming.shape, jnp.bfloat16)]
        + [pltpu.VMEM(gate_own.shape, jnp.bfloat16)] * 6
        + [pltpu.VMEM(incoming.shape, jnp.bfloat16), pltpu.SemaphoreType.DMA((PARTS + 7,))],
        compiler_params=limit(51),
        cost_estimate=pl.CostEstimate(
            flops=12 * incoming.size * gate_own.shape[0],
            transcendentals=2 * incoming.shape[0] * gate_own.shape[0],
            bytes_accessed=4 * incoming.size + 12 * gate_own.size,
        ),
    )(incoming, gate_own, up_own, down_own, gate_far, up_far, down_far)
    shares = lax.axis_size(TP)
    piece = model_width // shares
    leaving = partial.reshape(experts, half_slots, shares, piece)
    leaving = jnp.moveaxis(leaving, 2, 1).reshape(experts * shares, half_slots, piece)
    returned = lax.all_to_all(leaving, ALL, 0, 0, tiled=True)
    returned = returned.reshape(experts, shares // 2, 2, half_slots, piece)
    results = jnp.sum(returned.astype(jnp.float32), axis=1).astype(jnp.bfloat16)
    results = results.reshape(experts * capacity, piece)

    both = pl.pallas_call(
        blend_body,
        out_shape=jax.ShapeDtypeStruct((experts * capacity, 2 * row_count), jnp.bfloat16),
        compiler_params=limit(6),
    )(expert_choice.T, route_scores.T)
    mixed = lax.dot_general(
        both, results, (((0,), (0,)), ((), ())), preferred_element_type=jnp.float32
    )
    blended = (mixed[:row_count] + mixed[row_count:]).astype(jnp.bfloat16)

    whole = lax.all_gather(blended, TP)
    return jnp.transpose(whole, (1, 0, 2)).reshape(row_count, model_width), shard


def per_device(
    first_batch,
    mixer_gain,
    mixer_in,
    group_maps,
    pool_scale,
    mixer_out,
    second_batch,
    expert_gain,
    expert_choice,
    route_scores,
    expert_gate,
    expert_up,
    expert_down,
):
    experts_second, shard = expert_half(
        mixer_in,
        mixer_out,
        second_batch,
        expert_gain,
        expert_choice,
        route_scores,
        expert_gate,
        expert_up,
        expert_down,
    )
    groups, inner, outer = group_maps.shape
    same = jnp.eye(2, dtype=jnp.bfloat16)
    pair_maps = jnp.einsum("pgcd,gh->pgchd", group_maps.reshape(groups // 2, 2, inner, outer), same)
    pair_maps = pair_maps.reshape(groups // 2, 2 * inner, 2 * outer)
    mixed_first = mixer_half(first_batch, mixer_gain, shard, pair_maps, pool_scale)
    return (mixed_first, experts_second)


def solution(mesh):
    torus = Mesh(mesh.devices.reshape(8, 4, mesh.shape["tp"] // 2, 2), ALL)
    placed = (
        P(ALL, None),
        P(),
        P(None, TP),
        P(),
        P(),
        P(TP, None),
        P(EP, None),
        P(),
        P(EP, None),
        P(EP, None),
        P(EP, None, TP),
        P(EP, None, TP),
        P(EP, TP, None),
    )
    return jax.shard_map(
        per_device,
        mesh=torus,
        in_specs=placed,
        out_specs=(P(ALL, None), P(EP, None)),
        check_vma=False,
    )
```

```python
import jax
import jax.numpy as jnp
from jax import lax
from jax.experimental import pallas as pl
from jax.experimental.pallas import tpu as pltpu
from jax.sharding import Mesh
from jax.sharding import PartitionSpec as P

GROUP = 64
ALL = ("z", "x", "y", "c")
EP = ("z", "x")
TP = ("y", "c")
PARTS = 4
EXPERTS = 32
SWAP = [(0, 1), (1, 0)]

epsilon = 1e-06


def neighbours(block, width):
    count = lax.axis_size(ALL)
    forward = [(i, i + 1) for i in range(count - 1)]
    backward = [(target, source) for source, target in forward]
    low = lax.ppermute(block[block.shape[0] - width :], ALL, forward)
    high = lax.ppermute(block[:width], ALL, backward)
    return low, high


def in_place():
    return pl.BlockSpec(memory_space=pl.ANY)


def in_scalars():
    return pl.BlockSpec(memory_space=pltpu.SMEM)


def limit(mib):
    return pltpu.CompilerParams(vmem_limit_bytes=mib << 20)


def norm(values, gain):
    floats = values.astype(jnp.float32)
    factor = lax.rsqrt(jnp.mean(floats * floats, axis=-1, keepdims=True) + epsilon)
    return (floats * factor * gain).astype(jnp.bfloat16)


def fetch(blocks, half, rows, done):
    share = blocks.shape[1] // 2
    copies = []
    for k in range(blocks.shape[0]):
        copy = pltpu.make_async_copy(
            blocks.at[k, pl.ds(half * share, share), :],
            rows.at[pl.ds(k * share, share), :],
            done.at[k],
        )
        copy.start()
        copies.append(copy)
    return copies


def projected(rows, gain, in_rows):
    product = lax.dot_general(
        norm(rows, gain), in_rows, (((1,), (1,)), ((), ())), preferred_element_type=jnp.float32
    )
    return product.astype(jnp.bfloat16).astype(jnp.float32)


def mixer_body(place, gain, maps, scale, rows_from, low_from, high_from, blocks, out, *held):
    rows, low, high, in_rows, out_rows, done_rows, done_in, done_out = held
    copies = []
    for k, (source, target) in enumerate(((rows_from, rows), (low_from, low), (high_from, high))):
        copies.append(pltpu.make_async_copy(source, target, done_rows.at[k]))
        copies[-1].start()
    copies += fetch(blocks, 0, in_rows, done_in)
    later = fetch(blocks, 1, out_rows, done_out)
    for copy in copies:
        copy.wait()
    count_rows, channels = rows.shape[0], scale.shape[1]
    width = low.shape[0]
    pairs = maps.shape[0]
    lanes = maps.shape[1]
    weights = in_rows[...]
    edges = jnp.concatenate([low[...].astype(jnp.float32), high[...].astype(jnp.float32)], axis=0)
    edges = projected(edges, gain[...], weights)
    middle = projected(rows[...], gain[...], weights)
    sums = jnp.concatenate([edges[:width], middle, edges[width:]], axis=0)
    shape = (count_rows, channels)
    kind = lax.broadcasted_iota(jnp.int32, shape, 1) // GROUP % 4
    places = place[0] * count_rows + lax.broadcasted_iota(jnp.int32, shape, 0)
    length = place[1] * count_rows
    window_sum = jnp.zeros(shape, jnp.float32)
    for k in range(4):
        span = 1 << k
        kept = sums.shape[0] - span
        sums = sums[:kept] + sums[span:]
        window_sum = jnp.where(
            kind == k, sums[width - span : width - span + count_rows], window_sum
        )
    span = jnp.left_shift(jnp.ones(shape, jnp.int32), kind)
    window_count = jnp.minimum(places + span, length) - jnp.maximum(places - span, 0)
    centred = (window_sum / window_count.astype(jnp.float32) - middle).astype(jnp.bfloat16)
    pieces = []
    for k in range(pairs):
        lane = slice(k * lanes, (k + 1) * lanes)
        pieces.append((dot(centred[:, lane], maps[k]) * scale[:, lane]).astype(jnp.bfloat16))
    grouped = jnp.concatenate(pieces, axis=1)
    for copy in later:
        copy.wait()
    out[...] = dot(grouped, out_rows[...]).astype(jnp.bfloat16)


def mixer_half(first_batch, mixer_gain, shard, pair_maps, pool_scale):
    count_rows, width = first_batch.shape
    channels = pool_scale.shape[0]
    low, high = neighbours(first_batch, 8)
    blocks = lax.all_gather(shard, TP)
    place = jnp.stack([lax.axis_index(ALL), jnp.int32(lax.axis_size(ALL))]).astype(jnp.int32)
    whole = pl.BlockSpec()
    held = [(count_rows, width), low.shape, high.shape, (channels, width), (channels, width)]
    return pl.pallas_call(
        mixer_body,
        out_shape=jax.ShapeDtypeStruct((count_rows, width), jnp.bfloat16),
        in_specs=[in_scalars()] + [whole] * 3 + [in_place()] * 4,
        scratch_shapes=[pltpu.VMEM(shape, jnp.bfloat16) for shape in held]
        + [pltpu.SemaphoreType.DMA((n,)) for n in (3, blocks.shape[0], blocks.shape[0])],
        compiler_params=limit(59),
        cost_estimate=pl.CostEstimate(
            flops=4 * count_rows * width * channels,
            transcendentals=0,
            bytes_accessed=8 * channels * width,
        ),
    )(place, mixer_gain[None, :], pair_maps, pool_scale[None, :], first_batch, low, high, blocks)


def ranked(choice, experts):
    count = choice.shape[1]
    names = lax.broadcasted_iota(jnp.int32, (experts, count), 0)
    first = choice[0:1, :] == names
    second = choice[1:2, :] == names
    named = first | second
    rows = lax.broadcasted_iota(jnp.int32, (count, count), 0)
    others = lax.broadcasted_iota(jnp.int32, (count, count), 1)
    earlier = jnp.where(rows < others, 1.0, 0.0).astype(jnp.bfloat16)
    rank = dot(jnp.where(named, 1.0, 0.0).astype(jnp.bfloat16), earlier)
    return first, second, jnp.where(named, rank, -1.0).astype(jnp.bfloat16)


def repeated(values, repeats):
    experts = values.shape[0]
    shape = (experts * repeats, experts)
    owner = lax.broadcasted_iota(jnp.int32, shape, 0) // repeats
    match = owner == lax.broadcasted_iota(jnp.int32, shape, 1)
    return dot(jnp.where(match, 1.0, 0.0).astype(jnp.bfloat16), values)


def dispatch_body(core, rows_from, gain_from, choice_from, out, rows, gain, choice, done):
    copies = []
    for k, (source, held) in enumerate(
        ((choice_from, choice), (rows_from, rows), (gain_from, gain))
    ):
        copies.append(pltpu.make_async_copy(source, held, done.at[k]))
        copies[-1].start()
    count = rows.shape[0]
    slots = out.shape[0]
    half = slots // EXPERTS
    slot = core[0] * half + lax.broadcasted_iota(jnp.int32, (slots, count), 0) % half
    copies[0].wait()
    rank = repeated(ranked(choice[...], EXPERTS)[2], half)
    spread = jnp.where(rank == slot.astype(jnp.float32), 1.0, 0.0).astype(jnp.bfloat16)
    copies[1].wait()
    copies[2].wait()
    out[...] = dot(spread, norm(rows[...], gain[...])).astype(jnp.bfloat16)


def blend_body(choice, scores, out):
    count = choice.shape[1]
    slots = out.shape[0]
    first, second, rank = ranked(choice[...], EXPERTS)
    repeats = slots // EXPERTS
    weight = 1.0 / (1.0 + jnp.exp(scores[1:2, :] - scores[0:1, :]))
    weights = jnp.where(first, weight, jnp.where(second, 1.0 - weight, 0.0))
    high = weights.astype(jnp.bfloat16)
    low = (weights - high.astype(jnp.float32)).astype(jnp.bfloat16)
    slot = lax.broadcasted_iota(jnp.int32, (slots, count), 0) % repeats
    match = repeated(rank, repeats) == slot.astype(jnp.float32)
    out[:, :count] = jnp.where(match, repeated(high, repeats), 0.0).astype(jnp.bfloat16)
    out[:, count:] = jnp.where(match, repeated(low, repeats), 0.0).astype(jnp.bfloat16)


def ffn_body(*refs):
    sources, out, held, done = refs[:7], refs[7], refs[8:16], refs[16]
    fetches = []
    for k in range(7):
        fetches.append(pltpu.make_async_copy(sources[k], held[k], done.at[PARTS + k]))
        fetches[-1].start()
    rows, _, _, down_a, _, _, down_b, result = held
    fetches[0].wait()
    values = rows[...]

    def product(k):
        fetches[k].wait()
        return lax.dot_general(
            values, held[k][...], (((1,), (1,)), ((), ())), preferred_element_type=jnp.float32
        )

    def hidden(gate, up):
        return (gate / (1.0 + jnp.exp(-gate)) * up).astype(jnp.bfloat16)

    hidden_a = hidden(product(1), product(2))
    hidden_b = hidden(product(4), product(5))
    fetches[3].wait()
    fetches[6].wait()
    width = result.shape[1] // PARTS
    copies = []
    for k in range(PARTS):
        span = pl.ds(k * width, width)
        total = dot(hidden_a, down_a[:, span]) + dot(hidden_b, down_b[:, span])
        result[:, span] = total.astype(jnp.bfloat16)
        copies.append(pltpu.make_async_copy(result.at[:, span], out.at[:, span], done.at[k]))
        copies[-1].start()
    for copy in copies:
        copy.wait()


def dot(left, right):
    return jnp.dot(left, right, preferred_element_type=jnp.float32)


def expert_half(
    mixer_in,
    mixer_out,
    second_batch,
    expert_gain,
    expert_choice,
    route_scores,
    expert_gate,
    expert_up,
    expert_down,
):
    row_count, model_width = second_batch.shape
    experts = lax.axis_size(EP)
    capacity = 4 * row_count // experts
    half_slots = capacity // 2
    core = lax.axis_index("c")

    gate_own, up_own, down_own = expert_gate[0].T, expert_up[0].T, expert_down[0]
    gate_far = lax.ppermute(gate_own, "c", SWAP)
    up_far = lax.ppermute(up_own, "c", SWAP)
    down_far = lax.ppermute(down_own, "c", SWAP)

    outgoing = pl.pallas_call(
        dispatch_body,
        out_shape=jax.ShapeDtypeStruct((experts * half_slots, model_width), jnp.bfloat16),
        in_specs=[in_scalars()] + [in_place()] * 3,
        scratch_shapes=[
            pltpu.VMEM(second_batch.shape, second_batch.dtype),
            pltpu.VMEM((1, model_width), jnp.float32),
            pltpu.VMEM((expert_choice.shape[1], row_count), jnp.int32),
            pltpu.SemaphoreType.DMA((3,)),
        ],
        compiler_params=limit(61),
        cost_estimate=pl.CostEstimate(
            flops=2 * experts * half_slots * second_batch.size,
            transcendentals=row_count,
            bytes_accessed=6 * second_batch.size,
        ),
    )(core[None].astype(jnp.int32), second_batch, expert_gain[None, :], expert_choice.T)
    outgoing = outgoing.reshape(experts, half_slots, model_width)
    mixer_in, mixer_out, outgoing = lax.optimization_barrier((mixer_in, mixer_out, outgoing))
    shard = jnp.concatenate([mixer_in.T, mixer_out], axis=0)
    arrived = lax.all_to_all(outgoing, EP, 0, 0, tiled=True)
    incoming = arrived.reshape(experts * half_slots, model_width)

    partial = pl.pallas_call(
        ffn_body,
        out_shape=jax.ShapeDtypeStruct(incoming.shape, jnp.bfloat16),
        in_specs=[in_place()] * 7,
        out_specs=in_place(),
        scratch_shapes=[pltpu.VMEM(incoming.shape, jnp.bfloat16)]
        + [pltpu.VMEM(gate_own.shape, jnp.bfloat16)] * 6
        + [pltpu.VMEM(incoming.shape, jnp.bfloat16), pltpu.SemaphoreType.DMA((PARTS + 7,))],
        compiler_params=limit(51),
        cost_estimate=pl.CostEstimate(
            flops=12 * incoming.size * gate_own.shape[0],
            transcendentals=2 * incoming.shape[0] * gate_own.shape[0],
            bytes_accessed=4 * incoming.size + 12 * gate_own.size,
        ),
    )(incoming, gate_own, up_own, down_own, gate_far, up_far, down_far)
    shares = lax.axis_size(TP)
    piece = model_width // shares
    leaving = partial.reshape(experts, half_slots, shares, piece)
    leaving = jnp.moveaxis(leaving, 2, 1).reshape(experts * shares, half_slots, piece)
    returned = lax.all_to_all(leaving, ALL, 0, 0, tiled=True)
    returned = returned.reshape(experts, shares // 2, 2, half_slots, piece)
    results = jnp.sum(returned.astype(jnp.float32), axis=1).astype(jnp.bfloat16)
    results = results.reshape(experts * capacity, piece)

    both = pl.pallas_call(
        blend_body,
        out_shape=jax.ShapeDtypeStruct((experts * capacity, 2 * row_count), jnp.bfloat16),
        compiler_params=limit(6),
    )(expert_choice.T, route_scores.T)
    mixed = lax.dot_general(
        both, results, (((0,), (0,)), ((), ())), preferred_element_type=jnp.float32
    )
    blended = (mixed[:row_count] + mixed[row_count:]).astype(jnp.bfloat16)

    whole = lax.all_gather(blended, TP)
    return jnp.transpose(whole, (1, 0, 2)).reshape(row_count, model_width), shard


def per_device(
    first_batch,
    mixer_gain,
    mixer_in,
    group_maps,
    pool_scale,
    mixer_out,
    second_batch,
    expert_gain,
    expert_choice,
    route_scores,
    expert_gate,
    expert_up,
    expert_down,
):
    experts_second, shard = expert_half(
        mixer_in,
        mixer_out,
        second_batch,
        expert_gain,
        expert_choice,
        route_scores,
        expert_gate,
        expert_up,
        expert_down,
    )
    groups, inner, outer = group_maps.shape
    same = jnp.eye(2, dtype=jnp.bfloat16)
    pair_maps = jnp.einsum("pgcd,gh->pgchd", group_maps.reshape(groups // 2, 2, inner, outer), same)
    pair_maps = pair_maps.reshape(groups // 2, 2 * inner, 2 * outer)
    mixed_first = mixer_half(first_batch, mixer_gain, shard, pair_maps, pool_scale)
    return (mixed_first, experts_second)


def solution(mesh):
    torus = Mesh(mesh.devices.reshape(8, 4, mesh.shape["tp"] // 2, 2), ALL)
    placed = (
        P(ALL, None),
        P(),
        P(None, TP),
        P(),
        P(),
        P(TP, None),
        P(EP, None),
        P(),
        P(EP, None),
        P(EP, None),
        P(EP, None, TP),
        P(EP, None, TP),
        P(EP, TP, None),
    )
    return jax.shard_map(
        per_device,
        mesh=torus,
        in_specs=placed,
        out_specs=(P(ALL, None), P(EP, None)),
        check_vma=False,
    )
```

```python
import jax
import jax.numpy as jnp
from jax import lax
from jax.experimental import pallas as pl
from jax.experimental.pallas import tpu as pltpu
from jax.sharding import Mesh
from jax.sharding import PartitionSpec as P

GROUP = 64
ALL = ("z", "x", "y", "c")
EP = ("z", "x")
TP = ("y", "c")
PARTS = 4
EXPERTS = 32
SWAP = [(0, 1), (1, 0)]

epsilon = 1e-06


def neighbours(block, width):
    count = lax.axis_size(ALL)
    forward = [(i, i + 1) for i in range(count - 1)]
    backward = [(target, source) for source, target in forward]
    low = lax.ppermute(block[block.shape[0] - width :], ALL, forward)
    high = lax.ppermute(block[:width], ALL, backward)
    return low, high


def in_place():
    return pl.BlockSpec(memory_space=pl.ANY)


def in_scalars():
    return pl.BlockSpec(memory_space=pltpu.SMEM)


def limit(mib):
    return pltpu.CompilerParams(vmem_limit_bytes=mib << 20)


def norm(values, gain):
    floats = values.astype(jnp.float32)
    factor = lax.rsqrt(jnp.mean(floats * floats, axis=-1, keepdims=True) + epsilon)
    return (floats * factor * gain).astype(jnp.bfloat16)


def fetch(blocks, half, rows, done):
    share = blocks.shape[1] // 2
    copies = []
    for k in range(blocks.shape[0]):
        copy = pltpu.make_async_copy(
            blocks.at[k, pl.ds(half * share, share), :],
            rows.at[pl.ds(k * share, share), :],
            done.at[k],
        )
        copy.start()
        copies.append(copy)
    return copies


def projected(rows, gain, in_rows):
    product = lax.dot_general(
        norm(rows, gain), in_rows, (((1,), (1,)), ((), ())), preferred_element_type=jnp.float32
    )
    return product.astype(jnp.bfloat16).astype(jnp.float32)


def mixer_body(place, gain, maps, scale, rows_from, low_from, high_from, blocks, out, *held):
    rows, low, high, in_rows, out_rows, done_rows, done_in, done_out = held
    copies = []
    for k, (source, target) in enumerate(((rows_from, rows), (low_from, low), (high_from, high))):
        copies.append(pltpu.make_async_copy(source, target, done_rows.at[k]))
        copies[-1].start()
    copies += fetch(blocks, 0, in_rows, done_in)
    later = fetch(blocks, 1, out_rows, done_out)
    for copy in copies:
        copy.wait()
    count_rows, channels = rows.shape[0], scale.shape[1]
    width = low.shape[0]
    pairs = maps.shape[0]
    lanes = maps.shape[1]
    weights = in_rows[...]
    edges = jnp.concatenate([low[...].astype(jnp.float32), high[...].astype(jnp.float32)], axis=0)
    edges = projected(edges, gain[...], weights)
    middle = projected(rows[...], gain[...], weights)
    sums = jnp.concatenate([edges[:width], middle, edges[width:]], axis=0)
    shape = (count_rows, channels)
    kind = lax.broadcasted_iota(jnp.int32, shape, 1) // GROUP % 4
    places = place[0] * count_rows + lax.broadcasted_iota(jnp.int32, shape, 0)
    length = place[1] * count_rows
    window_sum = jnp.zeros(shape, jnp.float32)
    for k in range(4):
        span = 1 << k
        kept = sums.shape[0] - span
        sums = sums[:kept] + sums[span:]
        window_sum = jnp.where(
            kind == k, sums[width - span : width - span + count_rows], window_sum
        )
    span = jnp.left_shift(jnp.ones(shape, jnp.int32), kind)
    window_count = jnp.minimum(places + span, length) - jnp.maximum(places - span, 0)
    centred = (window_sum / window_count.astype(jnp.float32) - middle).astype(jnp.bfloat16)
    pieces = []
    for k in range(pairs):
        lane = slice(k * lanes, (k + 1) * lanes)
        pieces.append((dot(centred[:, lane], maps[k]) * scale[:, lane]).astype(jnp.bfloat16))
    grouped = jnp.concatenate(pieces, axis=1)
    for copy in later:
        copy.wait()
    out[...] = dot(grouped, out_rows[...]).astype(jnp.bfloat16)


def mixer_half(first_batch, mixer_gain, shard, pair_maps, pool_scale):
    count_rows, width = first_batch.shape
    channels = pool_scale.shape[0]
    low, high = neighbours(first_batch, 8)
    blocks = lax.all_gather(shard, TP)
    place = jnp.stack([lax.axis_index(ALL), jnp.int32(lax.axis_size(ALL))]).astype(jnp.int32)
    whole = pl.BlockSpec()
    held = [(count_rows, width), low.shape, high.shape, (channels, width), (channels, width)]
    return pl.pallas_call(
        mixer_body,
        out_shape=jax.ShapeDtypeStruct((count_rows, width), jnp.bfloat16),
        in_specs=[in_scalars()] + [whole] * 3 + [in_place()] * 4,
        scratch_shapes=[pltpu.VMEM(shape, jnp.bfloat16) for shape in held]
        + [pltpu.SemaphoreType.DMA((n,)) for n in (3, blocks.shape[0], blocks.shape[0])],
        compiler_params=limit(59),
        cost_estimate=pl.CostEstimate(
            flops=4 * count_rows * width * channels,
            transcendentals=0,
            bytes_accessed=8 * channels * width,
        ),
    )(place, mixer_gain[None, :], pair_maps, pool_scale[None, :], first_batch, low, high, blocks)


def ranked(choice, experts):
    count = choice.shape[1]
    names = lax.broadcasted_iota(jnp.int32, (experts, count), 0)
    first = choice[0:1, :] == names
    second = choice[1:2, :] == names
    named = first | second
    rows = lax.broadcasted_iota(jnp.int32, (count, count), 0)
    others = lax.broadcasted_iota(jnp.int32, (count, count), 1)
    earlier = jnp.where(rows < others, 1.0, 0.0).astype(jnp.bfloat16)
    rank = dot(jnp.where(named, 1.0, 0.0).astype(jnp.bfloat16), earlier)
    return first, second, jnp.where(named, rank, -1.0).astype(jnp.bfloat16)


def repeated(values, repeats):
    experts = values.shape[0]
    shape = (experts * repeats, experts)
    owner = lax.broadcasted_iota(jnp.int32, shape, 0) // repeats
    match = owner == lax.broadcasted_iota(jnp.int32, shape, 1)
    return dot(jnp.where(match, 1.0, 0.0).astype(jnp.bfloat16), values)


def dispatch_body(core, rows_from, gain_from, choice_from, top, bottom, *refs):
    out, joined, rows, gain, choice, result, done, left = refs
    share = top.shape[0]
    copies = []
    for k, (source, target) in enumerate(
        (
            (choice_from, choice),
            (rows_from, rows),
            (gain_from, gain),
            (top, joined.at[pl.ds(0, share), :]),
            (bottom, joined.at[pl.ds(share, share), :]),
        )
    ):
        copies.append(pltpu.make_async_copy(source, target, done.at[k]))
        copies[-1].start()
    count = rows.shape[0]
    slots = result.shape[0]
    half = slots // EXPERTS
    slot = core[0] * half + lax.broadcasted_iota(jnp.int32, (slots, count), 0) % half
    copies[0].wait()
    rank = repeated(ranked(choice[...], EXPERTS)[2], half)
    spread = jnp.where(rank == slot.astype(jnp.float32), 1.0, 0.0).astype(jnp.bfloat16)
    copies[1].wait()
    copies[2].wait()
    normed = norm(rows[...], gain[...])
    width = result.shape[1] // PARTS
    leaving = []
    for k in range(PARTS):
        span = slice(k * width, (k + 1) * width)
        result[:, span] = dot(spread, normed[:, span]).astype(jnp.bfloat16)
        lanes = pl.ds(k * width, width)
        leaving.append(pltpu.make_async_copy(result.at[:, lanes], out.at[:, lanes], left.at[k]))
        leaving[-1].start()
    for copy in copies[3:] + leaving:
        copy.wait()


def blend_body(choice, scores, out):
    count = choice.shape[1]
    slots = out.shape[0]
    first, second, rank = ranked(choice[...], EXPERTS)
    repeats = slots // EXPERTS
    weight = 1.0 / (1.0 + jnp.exp(scores[1:2, :] - scores[0:1, :]))
    weights = jnp.where(first, weight, jnp.where(second, 1.0 - weight, 0.0))
    high = weights.astype(jnp.bfloat16)
    low = (weights - high.astype(jnp.float32)).astype(jnp.bfloat16)
    slot = lax.broadcasted_iota(jnp.int32, (slots, count), 0) % repeats
    match = repeated(rank, repeats) == slot.astype(jnp.float32)
    out[:, :count] = jnp.where(match, repeated(high, repeats), 0.0).astype(jnp.bfloat16)
    out[:, count:] = jnp.where(match, repeated(low, repeats), 0.0).astype(jnp.bfloat16)


def ffn_body(*refs):
    sources, out, held, done = refs[:7], refs[7], refs[8:16], refs[16]
    fetches = []
    for k in range(7):
        fetches.append(pltpu.make_async_copy(sources[k], held[k], done.at[PARTS + k]))
        fetches[-1].start()
    rows, _, _, down_a, _, _, down_b, result = held
    fetches[0].wait()
    values = rows[...]

    def product(k):
        fetches[k].wait()
        return lax.dot_general(
            values, held[k][...], (((1,), (1,)), ((), ())), preferred_element_type=jnp.float32
        )

    def hidden(gate, up):
        return (gate / (1.0 + jnp.exp(-gate)) * up).astype(jnp.bfloat16)

    hidden_a = hidden(product(1), product(2))
    hidden_b = hidden(product(4), product(5))
    fetches[3].wait()
    fetches[6].wait()
    width = result.shape[1] // PARTS
    copies = []
    for k in range(PARTS):
        span = pl.ds(k * width, width)
        total = dot(hidden_a, down_a[:, span]) + dot(hidden_b, down_b[:, span])
        result[:, span] = total.astype(jnp.bfloat16)
        copies.append(pltpu.make_async_copy(result.at[:, span], out.at[:, span], done.at[k]))
        copies[-1].start()
    for copy in copies:
        copy.wait()


def dot(left, right):
    return jnp.dot(left, right, preferred_element_type=jnp.float32)


def expert_half(
    mixer_in,
    mixer_out,
    second_batch,
    expert_gain,
    expert_choice,
    route_scores,
    expert_gate,
    expert_up,
    expert_down,
):
    row_count, model_width = second_batch.shape
    experts = lax.axis_size(EP)
    capacity = 4 * row_count // experts
    half_slots = capacity // 2
    core = lax.axis_index("c")

    gate_own, up_own, down_own = expert_gate[0].T, expert_up[0].T, expert_down[0]
    gate_far = lax.ppermute(gate_own, "c", SWAP)
    up_far = lax.ppermute(up_own, "c", SWAP)
    down_far = lax.ppermute(down_own, "c", SWAP)

    joined_shape = (2 * mixer_out.shape[0], model_width)
    sent_shape = (experts * half_slots, model_width)
    outgoing, shard = pl.pallas_call(
        dispatch_body,
        out_shape=(
            jax.ShapeDtypeStruct(sent_shape, jnp.bfloat16),
            jax.ShapeDtypeStruct(joined_shape, jnp.bfloat16),
        ),
        in_specs=[in_scalars()] + [in_place()] * 5,
        out_specs=(in_place(), in_place()),
        scratch_shapes=[
            pltpu.VMEM(second_batch.shape, second_batch.dtype),
            pltpu.VMEM((1, model_width), jnp.float32),
            pltpu.VMEM((expert_choice.shape[1], row_count), jnp.int32),
            pltpu.VMEM(sent_shape, jnp.bfloat16),
            pltpu.SemaphoreType.DMA((5,)),
            pltpu.SemaphoreType.DMA((PARTS,)),
        ],
        compiler_params=limit(61),
        cost_estimate=pl.CostEstimate(
            flops=2 * experts * half_slots * second_batch.size,
            transcendentals=row_count,
            bytes_accessed=6 * second_batch.size,
        ),
    )(
        core[None].astype(jnp.int32),
        second_batch,
        expert_gain[None, :],
        expert_choice.T,
        mixer_in.T,
        mixer_out,
    )
    outgoing = outgoing.reshape(experts, half_slots, model_width)
    arrived = lax.all_to_all(outgoing, EP, 0, 0, tiled=True)
    incoming = arrived.reshape(experts * half_slots, model_width)

    partial = pl.pallas_call(
        ffn_body,
        out_shape=jax.ShapeDtypeStruct(incoming.shape, jnp.bfloat16),
        in_specs=[in_place()] * 7,
        out_specs=in_place(),
        scratch_shapes=[pltpu.VMEM(incoming.shape, jnp.bfloat16)]
        + [pltpu.VMEM(gate_own.shape, jnp.bfloat16)] * 6
        + [pltpu.VMEM(incoming.shape, jnp.bfloat16), pltpu.SemaphoreType.DMA((PARTS + 7,))],
        compiler_params=limit(57),
        cost_estimate=pl.CostEstimate(
            flops=12 * incoming.size * gate_own.shape[0],
            transcendentals=2 * incoming.shape[0] * gate_own.shape[0],
            bytes_accessed=4 * incoming.size + 12 * gate_own.size,
        ),
    )(incoming, gate_own, up_own, down_own, gate_far, up_far, down_far)
    shares = lax.axis_size(TP)
    piece = model_width // shares
    leaving = partial.reshape(experts, half_slots, shares, piece)
    leaving = jnp.moveaxis(leaving, 2, 1).reshape(experts * shares, half_slots, piece)
    returned = lax.all_to_all(leaving, ALL, 0, 0, tiled=True)
    returned = returned.reshape(experts, shares // 2, 2, half_slots, piece)
    results = jnp.sum(returned.astype(jnp.float32), axis=1).astype(jnp.bfloat16)
    results = results.reshape(experts * capacity, piece)

    both = pl.pallas_call(
        blend_body,
        out_shape=jax.ShapeDtypeStruct((experts * capacity, 2 * row_count), jnp.bfloat16),
        compiler_params=limit(6),
    )(expert_choice.T, route_scores.T)
    mixed = lax.dot_general(
        both, results, (((0,), (0,)), ((), ())), preferred_element_type=jnp.float32
    )
    blended = (mixed[:row_count] + mixed[row_count:]).astype(jnp.bfloat16)

    whole = lax.all_gather(blended, TP)
    return jnp.transpose(whole, (1, 0, 2)).reshape(row_count, model_width), shard


def per_device(
    first_batch,
    mixer_gain,
    mixer_in,
    group_maps,
    pool_scale,
    mixer_out,
    second_batch,
    expert_gain,
    expert_choice,
    route_scores,
    expert_gate,
    expert_up,
    expert_down,
):
    experts_second, shard = expert_half(
        mixer_in,
        mixer_out,
        second_batch,
        expert_gain,
        expert_choice,
        route_scores,
        expert_gate,
        expert_up,
        expert_down,
    )
    groups, inner, outer = group_maps.shape
    same = jnp.eye(2, dtype=jnp.bfloat16)
    pair_maps = jnp.einsum("pgcd,gh->pgchd", group_maps.reshape(groups // 2, 2, inner, outer), same)
    pair_maps = pair_maps.reshape(groups // 2, 2 * inner, 2 * outer)
    mixed_first = mixer_half(first_batch, mixer_gain, shard, pair_maps, pool_scale)
    return (mixed_first, experts_second)


def solution(mesh):
    torus = Mesh(mesh.devices.reshape(8, 4, mesh.shape["tp"] // 2, 2), ALL)
    placed = (
        P(ALL, None),
        P(),
        P(None, TP),
        P(),
        P(),
        P(TP, None),
        P(EP, None),
        P(),
        P(EP, None),
        P(EP, None),
        P(EP, None, TP),
        P(EP, None, TP),
        P(EP, TP, None),
    )
    return jax.shard_map(
        per_device,
        mesh=torus,
        in_specs=placed,
        out_specs=(P(ALL, None), P(EP, None)),
        check_vma=False,
    )
```

```python
import jax
import jax.numpy as jnp
from jax import lax
from jax.experimental import pallas as pl
from jax.experimental.pallas import tpu as pltpu
from jax.sharding import Mesh
from jax.sharding import PartitionSpec as P

GROUP = 64
ALL = ("z", "x", "y", "c")
EP = ("z", "x")
TP = ("y", "c")
PARTS = 4
EXPERTS = 32
SWAP = [(0, 1), (1, 0)]

epsilon = 1e-06


def neighbours(block, width):
    count = lax.axis_size(ALL)
    forward = [(i, i + 1) for i in range(count - 1)]
    backward = [(target, source) for source, target in forward]
    low = lax.ppermute(block[block.shape[0] - width :], ALL, forward)
    high = lax.ppermute(block[:width], ALL, backward)
    return low, high


def in_place():
    return pl.BlockSpec(memory_space=pl.ANY)


def in_scalars():
    return pl.BlockSpec(memory_space=pltpu.SMEM)


def limit(mib):
    return pltpu.CompilerParams(vmem_limit_bytes=mib << 20)


def norm(values, gain):
    floats = values.astype(jnp.float32)
    factor = lax.rsqrt(jnp.mean(floats * floats, axis=-1, keepdims=True) + epsilon)
    return (floats * factor * gain).astype(jnp.bfloat16)


def fetch(blocks, half, rows, done):
    share = blocks.shape[1] // 2
    copies = []
    for k in range(blocks.shape[0]):
        copy = pltpu.make_async_copy(
            blocks.at[k, pl.ds(half * share, share), :],
            rows.at[pl.ds(k * share, share), :],
            done.at[k],
        )
        copy.start()
        copies.append(copy)
    return copies


def projected(rows, gain, in_rows):
    product = lax.dot_general(
        norm(rows, gain), in_rows, (((1,), (1,)), ((), ())), preferred_element_type=jnp.float32
    )
    return product.astype(jnp.bfloat16).astype(jnp.float32)


def mixer_body(place, gain, maps, scale, rows_from, low_from, high_from, blocks, out, *held):
    rows, low, high, in_rows, out_rows, done_rows, done_in, done_out = held
    copies = []
    for k, (source, target) in enumerate(((rows_from, rows), (low_from, low), (high_from, high))):
        copies.append(pltpu.make_async_copy(source, target, done_rows.at[k]))
        copies[-1].start()
    copies += fetch(blocks, 0, in_rows, done_in)
    later = fetch(blocks, 1, out_rows, done_out)
    for copy in copies:
        copy.wait()
    count_rows, channels = rows.shape[0], scale.shape[1]
    width = low.shape[0]
    pairs = maps.shape[0]
    lanes = maps.shape[1]
    weights = in_rows[...]
    edges = jnp.concatenate([low[...].astype(jnp.float32), high[...].astype(jnp.float32)], axis=0)
    edges = projected(edges, gain[...], weights)
    middle = projected(rows[...], gain[...], weights)
    sums = jnp.concatenate([edges[:width], middle, edges[width:]], axis=0)
    shape = (count_rows, channels)
    kind = lax.broadcasted_iota(jnp.int32, shape, 1) // GROUP % 4
    places = place[0] * count_rows + lax.broadcasted_iota(jnp.int32, shape, 0)
    length = place[1] * count_rows
    window_sum = jnp.zeros(shape, jnp.float32)
    for k in range(4):
        span = 1 << k
        kept = sums.shape[0] - span
        sums = sums[:kept] + sums[span:]
        window_sum = jnp.where(
            kind == k, sums[width - span : width - span + count_rows], window_sum
        )
    span = jnp.left_shift(jnp.ones(shape, jnp.int32), kind)
    window_count = jnp.minimum(places + span, length) - jnp.maximum(places - span, 0)
    centred = (window_sum / window_count.astype(jnp.float32) - middle).astype(jnp.bfloat16)
    pieces = []
    for k in range(pairs):
        lane = slice(k * lanes, (k + 1) * lanes)
        pieces.append((dot(centred[:, lane], maps[k]) * scale[:, lane]).astype(jnp.bfloat16))
    grouped = jnp.concatenate(pieces, axis=1)
    for copy in later:
        copy.wait()
    out[...] = dot(grouped, out_rows[...]).astype(jnp.bfloat16)


def mixer_half(first_batch, mixer_gain, shard, pair_maps, pool_scale):
    count_rows, width = first_batch.shape
    channels = pool_scale.shape[0]
    low, high = neighbours(first_batch, 8)
    blocks = lax.all_gather(shard, TP)
    place = jnp.stack([lax.axis_index(ALL), jnp.int32(lax.axis_size(ALL))]).astype(jnp.int32)
    whole = pl.BlockSpec()
    held = [(count_rows, width), low.shape, high.shape, (channels, width), (channels, width)]
    return pl.pallas_call(
        mixer_body,
        out_shape=jax.ShapeDtypeStruct((count_rows, width), jnp.bfloat16),
        in_specs=[in_scalars()] + [whole] * 3 + [in_place()] * 4,
        scratch_shapes=[pltpu.VMEM(shape, jnp.bfloat16) for shape in held]
        + [pltpu.SemaphoreType.DMA((n,)) for n in (3, blocks.shape[0], blocks.shape[0])],
        compiler_params=limit(59),
        cost_estimate=pl.CostEstimate(
            flops=4 * count_rows * width * channels,
            transcendentals=0,
            bytes_accessed=8 * channels * width,
        ),
    )(place, mixer_gain[None, :], pair_maps, pool_scale[None, :], first_batch, low, high, blocks)


def ranked(choice, experts):
    count = choice.shape[1]
    names = lax.broadcasted_iota(jnp.int32, (experts, count), 0)
    first = choice[0:1, :] == names
    second = choice[1:2, :] == names
    named = first | second
    rows = lax.broadcasted_iota(jnp.int32, (count, count), 0)
    others = lax.broadcasted_iota(jnp.int32, (count, count), 1)
    earlier = jnp.where(rows < others, 1.0, 0.0).astype(jnp.bfloat16)
    rank = dot(jnp.where(named, 1.0, 0.0).astype(jnp.bfloat16), earlier)
    return first, second, jnp.where(named, rank, -1.0).astype(jnp.bfloat16)


def repeated(values, repeats):
    experts = values.shape[0]
    shape = (experts * repeats, experts)
    owner = lax.broadcasted_iota(jnp.int32, shape, 0) // repeats
    match = owner == lax.broadcasted_iota(jnp.int32, shape, 1)
    return dot(jnp.where(match, 1.0, 0.0).astype(jnp.bfloat16), values)


def dispatch_body(core, rows_from, gain_from, choice_from, out, *held):
    rows, gain, choice, result, done, left = held
    copies = []
    for k, (source, held) in enumerate(
        ((choice_from, choice), (rows_from, rows), (gain_from, gain))
    ):
        copies.append(pltpu.make_async_copy(source, held, done.at[k]))
        copies[-1].start()
    count = rows.shape[0]
    slots = result.shape[0]
    half = slots // EXPERTS
    slot = core[0] * half + lax.broadcasted_iota(jnp.int32, (slots, count), 0) % half
    copies[0].wait()
    rank = repeated(ranked(choice[...], EXPERTS)[2], half)
    spread = jnp.where(rank == slot.astype(jnp.float32), 1.0, 0.0).astype(jnp.bfloat16)
    copies[1].wait()
    copies[2].wait()
    normed = norm(rows[...], gain[...])
    width = result.shape[1] // PARTS
    leaving = []
    for k in range(PARTS):
        span = slice(k * width, (k + 1) * width)
        result[:, span] = dot(spread, normed[:, span]).astype(jnp.bfloat16)
        lanes = pl.ds(k * width, width)
        leaving.append(pltpu.make_async_copy(result.at[:, lanes], out.at[:, lanes], left.at[k]))
        leaving[-1].start()
    for copy in leaving:
        copy.wait()


def blend_body(choice, scores, out):
    count = choice.shape[1]
    slots = out.shape[0]
    first, second, rank = ranked(choice[...], EXPERTS)
    repeats = slots // EXPERTS
    weight = 1.0 / (1.0 + jnp.exp(scores[1:2, :] - scores[0:1, :]))
    weights = jnp.where(first, weight, jnp.where(second, 1.0 - weight, 0.0))
    high = weights.astype(jnp.bfloat16)
    low = (weights - high.astype(jnp.float32)).astype(jnp.bfloat16)
    slot = lax.broadcasted_iota(jnp.int32, (slots, count), 0) % repeats
    match = repeated(rank, repeats) == slot.astype(jnp.float32)
    out[:, :count] = jnp.where(match, repeated(high, repeats), 0.0).astype(jnp.bfloat16)
    out[:, count:] = jnp.where(match, repeated(low, repeats), 0.0).astype(jnp.bfloat16)


def ffn_body(*refs):
    sources, out, held, done = refs[:7], refs[7], refs[8:16], refs[16]
    fetches = []
    for k in range(7):
        fetches.append(pltpu.make_async_copy(sources[k], held[k], done.at[PARTS + k]))
        fetches[-1].start()
    rows, _, _, down_a, _, _, down_b, result = held
    fetches[0].wait()
    values = rows[...]

    def product(k):
        fetches[k].wait()
        return lax.dot_general(
            values, held[k][...], (((1,), (1,)), ((), ())), preferred_element_type=jnp.float32
        )

    def hidden(gate, up):
        return (gate / (1.0 + jnp.exp(-gate)) * up).astype(jnp.bfloat16)

    hidden_a = hidden(product(1), product(2))
    hidden_b = hidden(product(4), product(5))
    fetches[3].wait()
    fetches[6].wait()
    width = result.shape[1] // PARTS
    copies = []
    for k in range(PARTS):
        span = pl.ds(k * width, width)
        total = dot(hidden_a, down_a[:, span]) + dot(hidden_b, down_b[:, span])
        result[:, span] = total.astype(jnp.bfloat16)
        copies.append(pltpu.make_async_copy(result.at[:, span], out.at[:, span], done.at[k]))
        copies[-1].start()
    for copy in copies:
        copy.wait()


def dot(left, right):
    return jnp.dot(left, right, preferred_element_type=jnp.float32)


def expert_half(
    mixer_in,
    mixer_out,
    second_batch,
    expert_gain,
    expert_choice,
    route_scores,
    expert_gate,
    expert_up,
    expert_down,
):
    row_count, model_width = second_batch.shape
    experts = lax.axis_size(EP)
    capacity = 4 * row_count // experts
    half_slots = capacity // 2
    core = lax.axis_index("c")

    gate_own, up_own, down_own = expert_gate[0].T, expert_up[0].T, expert_down[0]
    gate_far = lax.ppermute(gate_own, "c", SWAP)
    up_far = lax.ppermute(up_own, "c", SWAP)
    down_far = lax.ppermute(down_own, "c", SWAP)

    outgoing = pl.pallas_call(
        dispatch_body,
        out_shape=jax.ShapeDtypeStruct((experts * half_slots, model_width), jnp.bfloat16),
        in_specs=[in_scalars()] + [in_place()] * 3,
        scratch_shapes=[
            pltpu.VMEM(second_batch.shape, second_batch.dtype),
            pltpu.VMEM((1, model_width), jnp.float32),
            pltpu.VMEM((expert_choice.shape[1], row_count), jnp.int32),
            pltpu.VMEM((experts * half_slots, model_width), jnp.bfloat16),
            pltpu.SemaphoreType.DMA((3,)),
            pltpu.SemaphoreType.DMA((PARTS,)),
        ],
        out_specs=in_place(),
        compiler_params=limit(61),
        cost_estimate=pl.CostEstimate(
            flops=2 * experts * half_slots * second_batch.size,
            transcendentals=row_count,
            bytes_accessed=6 * second_batch.size,
        ),
    )(core[None].astype(jnp.int32), second_batch, expert_gain[None, :], expert_choice.T)
    outgoing = outgoing.reshape(experts, half_slots, model_width)
    mixer_in, mixer_out, outgoing = lax.optimization_barrier((mixer_in, mixer_out, outgoing))
    shard = jnp.concatenate([mixer_in.T, mixer_out], axis=0)
    arrived = lax.all_to_all(outgoing, EP, 0, 0, tiled=True)
    incoming = arrived.reshape(experts * half_slots, model_width)

    partial = pl.pallas_call(
        ffn_body,
        out_shape=jax.ShapeDtypeStruct(incoming.shape, jnp.bfloat16),
        in_specs=[in_place()] * 7,
        out_specs=in_place(),
        scratch_shapes=[pltpu.VMEM(incoming.shape, jnp.bfloat16)]
        + [pltpu.VMEM(gate_own.shape, jnp.bfloat16)] * 6
        + [pltpu.VMEM(incoming.shape, jnp.bfloat16), pltpu.SemaphoreType.DMA((PARTS + 7,))],
        compiler_params=limit(51),
        cost_estimate=pl.CostEstimate(
            flops=12 * incoming.size * gate_own.shape[0],
            transcendentals=2 * incoming.shape[0] * gate_own.shape[0],
            bytes_accessed=4 * incoming.size + 12 * gate_own.size,
        ),
    )(incoming, gate_own, up_own, down_own, gate_far, up_far, down_far)
    shares = lax.axis_size(TP)
    piece = model_width // shares
    leaving = partial.reshape(experts, half_slots, shares, piece)
    leaving = jnp.moveaxis(leaving, 2, 1).reshape(experts * shares, half_slots, piece)
    returned = lax.all_to_all(leaving, ALL, 0, 0, tiled=True)
    returned = returned.reshape(experts, shares // 2, 2, half_slots, piece)
    results = jnp.sum(returned.astype(jnp.float32), axis=1).astype(jnp.bfloat16)
    results = results.reshape(experts * capacity, piece)

    both = pl.pallas_call(
        blend_body,
        out_shape=jax.ShapeDtypeStruct((experts * capacity, 2 * row_count), jnp.bfloat16),
        compiler_params=limit(6),
    )(expert_choice.T, route_scores.T)
    mixed = lax.dot_general(
        both, results, (((0,), (0,)), ((), ())), preferred_element_type=jnp.float32
    )
    blended = (mixed[:row_count] + mixed[row_count:]).astype(jnp.bfloat16)

    whole = lax.all_gather(blended, TP)
    return jnp.transpose(whole, (1, 0, 2)).reshape(row_count, model_width), shard


def per_device(
    first_batch,
    mixer_gain,
    mixer_in,
    group_maps,
    pool_scale,
    mixer_out,
    second_batch,
    expert_gain,
    expert_choice,
    route_scores,
    expert_gate,
    expert_up,
    expert_down,
):
    experts_second, shard = expert_half(
        mixer_in,
        mixer_out,
        second_batch,
        expert_gain,
        expert_choice,
        route_scores,
        expert_gate,
        expert_up,
        expert_down,
    )
    groups, inner, outer = group_maps.shape
    same = jnp.eye(2, dtype=jnp.bfloat16)
    pair_maps = jnp.einsum("pgcd,gh->pgchd", group_maps.reshape(groups // 2, 2, inner, outer), same)
    pair_maps = pair_maps.reshape(groups // 2, 2 * inner, 2 * outer)
    mixed_first = mixer_half(first_batch, mixer_gain, shard, pair_maps, pool_scale)
    return (mixed_first, experts_second)


def solution(mesh):
    torus = Mesh(mesh.devices.reshape(8, 4, mesh.shape["tp"] // 2, 2), ALL)
    placed = (
        P(ALL, None),
        P(),
        P(None, TP),
        P(),
        P(),
        P(TP, None),
        P(EP, None),
        P(),
        P(EP, None),
        P(EP, None),
        P(EP, None, TP),
        P(EP, None, TP),
        P(EP, TP, None),
    )
    return jax.shard_map(
        per_device,
        mesh=torus,
        in_specs=placed,
        out_specs=(P(ALL, None), P(EP, None)),
        check_vma=False,
    )
```
